32 devices in a mesh: ep: 4 (over y, x), tp: 8 (over z, core).
Axes of the slice: x: 2, y: 2, z: 4, core: 2. Of those that a mesh axis runs over, the one named last changes fastest.
Arguments:
- queries: bfloat16 [2048, 16, 128], P('ep', 'tp'), may hold values from -125 to 125
- keys: bfloat16 [2048, 16, 128], P('ep', 'tp'), may hold values from -9 to 9
- values: bfloat16 [2048, 16, 128], P('ep', 'tp'), may hold values from -6 to 6
- mixing: float32 [16], P('tp'), may hold values from 0.3 to 0.8
- head_gain: float32 [128], replicated, may hold values from 0.1 to 1.9
- out_weight: bfloat16 [16, 128, 2048], P('tp'), may hold values from -0.125 to 0.125
- tokens_b: bfloat16 [4096, 2048], P(('ep', 'tp')), may hold values from -6 to 6
- norm_gain: float32 [2048], replicated, may hold values from 0.1 to 1.9
- expert_ids: int32 [4096, 2], P(('ep', 'tp')), may hold values from 0 to 3, all different within a row; in each aligned block of 128 rows (0 to 127, 128 to 255, ...) at most 96 rows name the same one
- group_gate: float32 [4096], P(('ep', 'tp')), may hold values from 0.2 to 1
- expert_gate: float32 [4096, 2], P(('ep', 'tp')), may hold values from 0.1 to 0.9
- gate_weight: bfloat16 [4, 2048, 1024], P('ep', None, 'tp'), may hold values from -0.125 to 0.125
- up_weight: bfloat16 [4, 2048, 1024], P('ep', None, 'tp'), may hold values from -0.125 to 0.125
- down_weight: bfloat16 [4, 2048, 1024], P('ep', None, 'tp'), may hold values from -0.1875 to 0.1875
Outputs:
- mixed: bfloat16 [2048, 2048], P(('ep', 'tp'))
- routed: bfloat16 [4096, 2048], P(('ep', 'tp'))
The draws below stay inside these ranges and needn't reach their ends.
Inputs may be any that keep to these rules, and one draw needn't show every extreme that they name: `expert_ids`: within each aligned block of 128 rows, no expert is named by more than 96 rows, and some block has an expert named by exactly 96 rows.
All inputs are finite; a program needn't handle non-finite values.
Results may differ from the reference program's by a relative error of at most 0.019.
Values may be sent and summed in bfloat16 or wider, within the bound.
A program may use at most 192 MiB of HBM per device.

```python
import math
import jax
import jax.numpy as jnp
import numpy as np
from jax import lax

D = 2048
HEADS = 16
HEAD = 64
VAL = 128
FF = 1024
TOP = 2
EXPERTS = 4
SEQ_DEV = 512
LENGTH = 2048
TOK_DEV = 128
TOKENS_B = 4096
CAP = 96
N_EP = 4
N_TP = 8


def paired_fields(key):
    query_seed = jax.random.fold_in(key, 11)
    key_seed = jax.random.fold_in(key, 12)
    query_field = jnp.clip(jax.random.normal(query_seed, (LENGTH, HEADS, 2 * HEAD), jnp.float32), -5.0, 5.0)
    key_field = 1.75 * jnp.clip(jax.random.normal(key_seed, (LENGTH, HEADS, 2 * HEAD), jnp.float32), -5.0, 5.0)
    return (query_field, key_field)


def draw_queries(key, part):
    return paired_fields(key)[0].astype(jnp.bfloat16)


def draw_keys(key, part):
    return paired_fields(key)[1].astype(jnp.bfloat16)


def levels(rng, shape, pieces, smallest, top_value):
    level = 1.0
    for axis_at, parts in pieces:
        heights = jax.random.uniform(jax.random.fold_in(jax.random.fold_in(rng, 6), axis_at), (parts,), jnp.float32, smallest / len(pieces), top_value / len(pieces))
        level = level * jnp.repeat(jnp.exp(heights), shape[axis_at] // parts).reshape((-1,) + (1,) * (len(shape) - 1 - axis_at))
    return level


def shared_out(key, own, number, rows, count, top, most, lean):
    ranking = jax.random.permutation(key, count)
    packed, common = load_shares(count, rows * top, most, lean, True), load_shares(count, rows * top, most, lean, False)
    places = jnp.arange(count)

    def named(lengths, offset_by):
        used = int((lengths > 0).sum())
        fixed = max(1, used // 4)
        moved = fixed + (places - fixed + offset_by * (used - fixed)) % max(1, count - fixed)
        return jnp.zeros((count,), jnp.int32).at[ranking[jnp.where(places < fixed, places, moved)]].set(jnp.asarray(lengths, jnp.int32))

    lengths = jnp.where(number % 4 == 0, named(packed, number // 4), named(common, number - number // 4 - 1))
    mixed = jax.random.permutation(jax.random.fold_in(own, 3), count)
    source_of, taker = mixed[0:count // 2 * 2:2], mixed[1:count // 2 * 2:2]
    margin = jnp.minimum(lengths[source_of] - 1, most - lengths[taker]) // 2
    margin = jnp.where((source_of == ranking[0]) | (taker == ranking[0]) | (lengths[taker] == 0), 0, jnp.maximum(margin, 0))
    moved = jax.random.randint(jax.random.fold_in(own, 4), (count // 2,), 0, 1 << 20) % (margin + 1)
    lengths = lengths.at[source_of].add(-moved).at[taker].add(moved)
    items = jnp.searchsorted(jnp.cumsum(lengths), jnp.arange(rows * top), side="right").astype(jnp.int32)
    table = items.reshape(top, rows).T
    table = table[jax.random.permutation(jax.random.fold_in(own, 1), rows)]
    offset_by = jax.random.randint(jax.random.fold_in(own, 2), (rows, 1), 0, top)
    return jnp.take_along_axis(table, (jnp.arange(top)[None, :] + offset_by) % top, axis=1)


def load_shares(count, total, bound, lean, full):
    loads = [(1 << 20) // math.isqrt(standing ** lean) + 1 for standing in range(1, count + 1)]
    largest = bound if full else min(bound, max(-(-total // count), total * loads[0] // sum(loads)))
    least = 1 if total - largest >= count - 1 else 0
    given, spare = [largest] + [least] * (count - 1), total - largest - least * (count - 1)
    while spare > 0:
        free = [i for i in range(1, count) if given[i] < largest] or [i for i in range(1, count) if given[i] < bound]
        pool, budget = sum([loads[i] for i in free]), spare
        for i in free:
            extra = min(bound - given[i], max(1, budget * loads[i] // pool), spare)
            given[i] = given[i] + extra
            spare = spare - extra
    return np.array(given)


def scatter_about(stream_key, shape, scale, limit, cuts=(), kind=jnp.bfloat16):
    factor_of = levels(stream_key, shape, cuts, -0.22, 0.18) if cuts else 1.0
    array = jax.random.normal(stream_key, shape, jnp.float32) * scale * factor_of
    return jnp.minimum(jnp.maximum(array, -limit), limit).astype(kind)


def setup_inputs(seed: int = 0) -> dict:
    arg_keys = jax.random.split(jax.random.key(seed), 15)
    queries = draw_queries(jax.random.fold_in(arg_keys[14], 71), 0)
    keys = draw_keys(jax.random.fold_in(arg_keys[14], 71), 0)
    values = scatter_about(arg_keys[2], (LENGTH, HEADS, VAL), 1.0, 6.0, ((0, 4), (1, 8)))
    mixing = jnp.clip(0.3 + 0.5 * jax.random.uniform(arg_keys[3], (HEADS,), jnp.float32) ** levels(arg_keys[3], (HEADS,), ((0, 8),), -0.2, 0.2), 0.3, 0.8)
    head_gain = jnp.clip(1.0 + 0.18 * jax.random.normal(arg_keys[4], (VAL,), jnp.float32), 0.1, 1.9)
    out_weight = scatter_about(arg_keys[5], (HEADS, VAL, D), (HEADS * VAL) ** -0.5, 0.125, ((0, 8),))
    tokens_b = scatter_about(arg_keys[6], (TOKENS_B, D), 1.0, 6.0, ((0, 32),))
    norm_gain = jnp.clip(1.0 + 0.18 * jax.random.normal(arg_keys[7], (D,), jnp.float32), 0.1, 1.9)
    expert_ids_keys = jax.random.split(jax.random.fold_in(arg_keys[8], 1), TOKENS_B // TOK_DEV)
    expert_ids_turns = jax.random.permutation(jax.random.fold_in(arg_keys[8], 3), TOKENS_B // TOK_DEV)
    expert_ids = jax.vmap(lambda own, number: shared_out(jax.random.fold_in(arg_keys[8], 2), own, number, TOK_DEV, EXPERTS, TOP, CAP, 0))(expert_ids_keys, expert_ids_turns).reshape((TOKENS_B, TOP))
    group_gate = jnp.clip(jnp.exp(math.log(1.0) - 1.609438 * jax.random.uniform(arg_keys[9], (TOKENS_B,), jnp.float32) ** levels(arg_keys[9], (TOKENS_B,), ((0, 32),), -0.2, 0.2)), 0.2, 1.0)
    expert_gate = jnp.clip(0.1 + 0.79999997 * jax.random.uniform(arg_keys[10], (TOKENS_B, TOP), jnp.float32) ** levels(arg_keys[10], (TOKENS_B, TOP), ((0, 32),), -0.2, 0.2), 0.1, 0.9)
    gate_weight = scatter_about(arg_keys[11], (EXPERTS, D, FF), D ** -0.5, 0.125, ((0, 4), (2, 8)))
    up_weight = scatter_about(arg_keys[12], (EXPERTS, D, FF), D ** -0.5, 0.125, ((0, 4), (2, 8)))
    down_weight = scatter_about(arg_keys[13], (EXPERTS, D, FF), FF ** -0.5, 0.1875, ((0, 4), (2, 8)))
    return dict(queries=queries, keys=keys, values=values, mixing=mixing, head_gain=head_gain, out_weight=out_weight, tokens_b=tokens_b, norm_gain=norm_gain, expert_ids=expert_ids, group_gate=group_gate, expert_gate=expert_gate, gate_weight=gate_weight, up_weight=up_weight, down_weight=down_weight)


def attend_head(inputs, head_gain):
    query_head, key_head, value_head, weight_two = inputs
    positions = lax.iota(jnp.int32, LENGTH)
    score_scale = 1.0 / math.sqrt(HEAD)

    def one_block(block_index):
        query_block = lax.dynamic_slice_in_dim(query_head, block_index * SEQ_DEV, SEQ_DEV, 0)
        query_pos = block_index * SEQ_DEV + lax.iota(jnp.int32, SEQ_DEV)
        allowed = positions[None, :] <= query_pos[:, None]
        results = []
        for map_index in range(2):
            offset = map_index * HEAD
            scores = jnp.dot(query_block[:, offset:offset + HEAD], key_head[:, offset:offset + HEAD].T, preferred_element_type=jnp.float32) * score_scale
            scores = jnp.where(allowed, scores, -1e+30)
            row_top = lax.optimization_barrier(jnp.max(scores, axis=1, keepdims=True))
            expo = jnp.exp(scores - row_top)
            row_sum = lax.optimization_barrier(jnp.sum(expo, axis=1, keepdims=True))
            numerator = jnp.dot(expo.astype(jnp.bfloat16), value_head, preferred_element_type=jnp.float32)
            results.append(numerator / row_sum)
        diff = results[0] - weight_two * results[1]
        normed = diff * lax.rsqrt(lax.optimization_barrier(jnp.mean(diff * diff, axis=1, keepdims=True)) + 1e-05) * head_gain
        return normed.astype(jnp.bfloat16)
    blocks = lax.map(one_block, jnp.arange(N_EP, dtype=jnp.int32))
    return blocks.reshape(LENGTH, VAL)

def expert_apply(inputs):
    expert_rows, w_gate, w_up, w_down = inputs
    gate_part = jnp.dot(expert_rows, w_gate, preferred_element_type=jnp.float32)
    up_part = jnp.dot(expert_rows, w_up, preferred_element_type=jnp.float32)
    hidden = (jax.nn.silu(gate_part) * up_part).astype(jnp.bfloat16)
    return jnp.dot(hidden, w_down.T, preferred_element_type=jnp.float32).astype(jnp.bfloat16)

def block_slots(block_ids):
    one_hot = (block_ids[:, None] == jnp.arange(EXPERTS, dtype=jnp.int32)[None, :]).astype(jnp.int32)
    slot_rank = lax.optimization_barrier(jnp.sum((jnp.cumsum(one_hot, axis=0) - one_hot) * one_hot, axis=1))
    slot_index = block_ids * CAP + slot_rank
    owners = jnp.full((EXPERTS * CAP,), TOK_DEV, jnp.int32)
    owners = owners.at[slot_index].set(jnp.arange(TOK_DEV * TOP, dtype=jnp.int32) // TOP)
    return (slot_index, owners)

def reference(queries, keys, values, mixing, head_gain, out_weight, tokens_b, norm_gain, expert_ids, group_gate, expert_gate, gate_weight, up_weight, down_weight):
    attended = lax.map(lambda inputs: attend_head(inputs, head_gain), (jnp.transpose(queries, (1, 0, 2)), jnp.transpose(keys, (1, 0, 2)), jnp.transpose(values, (1, 0, 2)), mixing))
    group_heads = HEADS // N_TP
    summed = jnp.zeros((LENGTH, D), jnp.float32)
    for group in range(N_TP):
        lower_head = group * group_heads
        part = jnp.einsum('hqe,hed->qd', attended[lower_head:lower_head + group_heads].astype(jnp.float32), out_weight[lower_head:lower_head + group_heads].astype(jnp.float32))
        rounded = lax.optimization_barrier(part.astype(jnp.bfloat16))
        summed = summed + rounded.astype(jnp.float32)
    mixed = summed.astype(jnp.bfloat16)
    tokens_f = tokens_b.astype(jnp.float32)
    normed = (tokens_f * lax.rsqrt(lax.optimization_barrier(jnp.mean(tokens_f * tokens_f, axis=1, keepdims=True)) + 1e-06) * norm_gain).astype(jnp.bfloat16)
    block_count = N_EP * N_TP
    slot_index, owners = jax.vmap(block_slots)(expert_ids.reshape(block_count, TOK_DEV * TOP))
    padded = jnp.concatenate([normed.reshape(block_count, TOK_DEV, D), jnp.zeros((block_count, 1, D), jnp.bfloat16)], axis=1)
    buffers = jnp.take_along_axis(padded, owners[:, :, None], axis=1)
    per_expert = jnp.transpose(buffers.reshape(block_count, EXPERTS, CAP, D), (1, 0, 2, 3))
    per_expert = per_expert.reshape(EXPERTS, block_count * CAP, D)
    results = lax.map(expert_apply, (per_expert, gate_weight, up_weight, down_weight))
    results = jnp.transpose(results.reshape(EXPERTS, block_count, CAP, D), (1, 0, 2, 3))
    results = results.reshape(block_count, EXPERTS * CAP, D)
    picked = jnp.take_along_axis(results, slot_index[:, :, None], axis=1)
    picked = picked.reshape(TOKENS_B, TOP, D).astype(jnp.float32)
    route_weight = group_gate[:, None] * expert_gate
    routed = lax.optimization_barrier(jnp.sum(route_weight[:, :, None] * picked, axis=1)).astype(jnp.bfloat16)
    return (mixed, routed)
```

```python
import functools
import math

import jax
import jax.numpy as jnp
from jax import lax
from jax.experimental import pallas as pl
from jax.experimental.pallas import tpu as pltpu
from jax.sharding import PartitionSpec as P

HEAD = 64
CHUNKS = 4
PIECES = 2
RANKS = 16
F32 = jnp.float32
BF16 = jnp.bfloat16
MESH = pl.DeviceIdType.MESH
NT = (((1,), (1,)), ((), ()))
TN = (((0,), (0,)), ((), ()))


def kernel(
    ep,
    tp,
    mix_ref,
    q_ref,
    kv_ref,
    gain_ref,
    ow_ref,
    tok_ref,
    norm_ref,
    ids_ref,
    group_ref,
    gates_ref,
    gate_ref,
    up_ref,
    dn_ref,
    mixed_ref,
    routed_ref,
    kv_all,
    w_gu,
    w_dn,
    rows_x,
    out_ref,
    nrm,
    rank_ref,
    hid,
    back,
    ret,
    top_ref,
    sum_ref,
    val_ref,
    att,
    part,
    pair,
    chip_sum,
    landed,
    line_out,
    place_ref,
    route_ref,
    local_sem,
    kv_s,
    kv_r,
    t_s,
    t_r,
    x_s,
    x_r,
    gu_s,
    gu_r,
    sg_s,
    sg_r,
    dn_s,
    dn_r,
    sd_s,
    sd_r,
    h_s,
    h_r,
    pr_s,
    pr_r,
    rs_s,
    rs_r,
    b_s,
    b_r,
):
    chips = tp // 2
    me = lax.axis_index("ep")
    mine = lax.axis_index("tp")
    z = mine // 2
    core = mine % 2
    other = z * 2 + 1 - core
    inward = 1 - 2 * (z // (chips // 2))
    heads, length, wide = q_ref.shape
    local_rows, width = tok_ref.shape
    half = rows_x.shape[0] // 2
    cap = half // ep
    step = w_dn.shape[3]
    lanes = w_gu.shape[2] // 2
    unit = lanes // 2
    subs = w_dn.shape[1]
    deep = width // PIECES
    joined = gate_ref.shape[1] != unit
    inner = (z >= 1) & (z <= chips - 2)
    is_end = (z == 0) | (z == chips - 1)
    has_guest = (z == 1) | (z == chips - 2)

    def remote(src, dst, send, recv, target):
        return pltpu.make_async_remote_copy(
            src_ref=src,
            dst_ref=dst,
            send_sem=send,
            recv_sem=recv,
            device_id=target,
            device_id_type=MESH,
        )

    if joined:
        own_gu = [pltpu.make_async_copy(gate_ref, w_gu.at[z, :, pl.ds(0, lanes)], local_sem.at[0])]
    else:
        own_gu = [
            pltpu.make_async_copy(gate_ref, w_gu.at[z, :, pl.ds(0, unit)], local_sem.at[0]),
            pltpu.make_async_copy(up_ref, w_gu.at[z, :, pl.ds(unit, unit)], local_sem.at[1]),
        ]
    if subs == 1:
        own_dn = pltpu.make_async_copy(dn_ref, w_dn.at[z, 0, :, :, pl.ds(0, unit)], local_sem.at[2])
    else:
        own_dn = pltpu.make_async_copy(dn_ref, w_dn.at[z, 0], local_sem.at[2])
    for copy in own_gu:
        copy.start()
    own_dn.start()

    barrier = pltpu.get_barrier_semaphore()
    for s in range(1, ep):
        pl.semaphore_signal(
            barrier, inc=1, device_id={"ep": (me + s) % ep}, device_id_type=MESH
        )
    for s in range(1, tp):
        pl.semaphore_signal(
            barrier, inc=1, device_id={"tp": (mine + s) % tp}, device_id_type=MESH
        )
    pl.semaphore_wait(barrier, ep + tp - 2)

    def on_line(at):
        return (at >= 0) & (at <= chips - 1)

    def wants_gu(at):
        return (at >= 1) & (at <= chips - 2)

    def gu_part(src, j):
        return w_gu.at[src, pl.ds(j * deep, deep), pl.ds(0, lanes)]

    def gu_copy(src, j, way):
        return remote(
            gu_part(src, j),
            gu_part(src, j),
            gu_s.at[(1 - way) // 2, src, j],
            gu_r.at[src, j],
            {"tp": (z + way) * 2 + core},
        )

    def sg_copy(src, j):
        return remote(
            gu_part(src, j),
            w_gu.at[src, pl.ds(j * deep, deep), pl.ds(lanes, lanes)],
            sg_s.at[src, j],
            sg_r.at[src, j],
            {"tp": other},
        )

    def dn_part(src, c, which):
        if subs == 1:
            return w_dn.at[src, 0, c, :, pl.ds(which * unit, unit)]
        return w_dn.at[src, which, c]

    def dn_copy(src, c, way):
        return remote(
            dn_part(src, c, 0),
            dn_part(src, c, 0),
            dn_s.at[(1 - way) // 2, src, c],
            dn_r.at[src, c],
            {"tp": (z + way) * 2 + core},
        )

    def sd_copy(src, c):
        return remote(
            dn_part(src, c, 0), dn_part(src, c, 1), sd_s.at[src, c], sd_r.at[src, c], {"tp": other}
        )

    def start_own():
        for copy in own_gu:
            copy.wait()
        for way in (inward, -inward):

            @pl.when(wants_gu(z + way))
            def _(way=way):
                for j in range(PIECES):
                    gu_copy(z, j, way).start()

        own_dn.wait()
        for way in (inward, -inward):

            @pl.when(on_line(z + way))
            def _(way=way):
                for c in range(CHUNKS):
                    dn_copy(z, c, way).start()

        @pl.when(inner)
        def _():
            for j in range(PIECES):
                sg_copy(z, j).start()

        for c in range(CHUNKS):
            sd_copy(z, c).start()

    def source(k, near):
        return (z + k * inward, -inward) if near else (z - k * inward, inward)

    def pass_gu(k, near):
        src, way = source(k, near)

        @pl.when(inner & on_line(src))
        def _():
            for j in range(PIECES):
                gu_copy(src, j, way).wait_recv()
                pl.when(wants_gu(z + way))(lambda j=j: gu_copy(src, j, way).start())
                sg_copy(src, j).start()

    def ready_gu(src):
        for j in range(PIECES):
            sg_copy(src, j).wait_recv()

    def pass_dn(k, near, c):
        src, way = source(k, near)

        @pl.when(on_line(src))
        def _():
            dn_copy(src, c, way).wait_recv()
            pl.when(on_line(z + way))(lambda: dn_copy(src, c, way).start())
            sd_copy(src, c).start()

    def kv_copy(s):
        return remote(kv_ref, kv_all.at[s], kv_s.at[s], kv_r.at[s], {"ep": lax.rem(me + s, ep)})

    def send_kv():
        for s in range(1, ep):
            pl.when(me + s < ep)(lambda s=s: kv_copy(s).start())

    pl.when(inner)(start_own)
    pl.when(is_end)(send_kv)

    relative = ids_ref[...] - me
    relative = jnp.where(relative < 0, relative + ep, relative)
    table = (RANKS, local_rows)
    expert_row = lax.broadcasted_iota(jnp.int32, table, 0)
    named = jnp.zeros(table, F32)
    route = jnp.zeros(table, F32)
    for k in range(ids_ref.shape[0]):
        hit = expert_row == relative[k : k + 1, :]
        named = jnp.where(hit, 1.0, named)
        route = route + jnp.where(hit, group_ref[...] * gates_ref[k : k + 1, :], 0.0)
    square = (local_rows, local_rows)
    row_at = lax.broadcasted_iota(jnp.int32, square, 0)
    col_at = lax.broadcasted_iota(jnp.int32, square, 1)
    before = jnp.where(row_at < col_at, 1.0, 0.0).astype(BF16)
    rank = jnp.dot(named.astype(BF16), before, preferred_element_type=F32)
    rank_ref[0] = jnp.where(named > 0.5, rank, -1.0)
    tokens = tok_ref[...].astype(F32)
    nrm[0] = (
        tokens
        * lax.rsqrt(jnp.mean(tokens * tokens, axis=1, keepdims=True) + 1e-06)
        * norm_ref[...]
    ).astype(BF16)

    def guest_copies():
        target = {"tp": (z + inward) * 2 + core}
        return (
            remote(nrm.at[0], nrm.at[1], t_s.at[0], t_r.at[0], target),
            remote(rank_ref.at[0], rank_ref.at[1], t_s.at[1], t_r.at[1], target),
        )

    @pl.when(is_end)
    def _():
        for copy in guest_copies():
            copy.start()
        start_own()

    def x_copy(g, s):
        return remote(
            out_ref.at[g, s - 1],
            rows_x.at[pl.ds(g * half + s * cap, cap)],
            x_s.at[g, s],
            x_r.at[g, s],
            {"ep": lax.rem(me + s, ep)},
        )

    slot_row = lax.broadcasted_iota(jnp.int32, (cap, local_rows), 0).astype(F32)

    def place_of(g, s):
        return jnp.where(rank_ref[g, s : s + 1, :] == slot_row, 1.0, 0.0).astype(BF16)

    def dispatch(g):
        for s in list(range(1, ep)) + [0]:
            place = place_of(g, s)
            for n in range(CHUNKS):
                cols = slice(n * step, (n + 1) * step)
                picked = jnp.dot(place, nrm[g, :, cols], preferred_element_type=F32).astype(BF16)
                if s:
                    out_ref[g, s - 1, :, cols] = picked
                else:
                    rows_x[g * half : g * half + cap, cols] = picked
            if s:
                x_copy(g, s).start()

    pl.when(inner)(lambda: dispatch(0))

    tile = min(256, length)
    tiles = length // tile

    def attend(s):
        block = kv_ref if s == 0 else kv_all.at[s]

        def one(index, carry):
            h = index // tiles
            start = pl.multiple_of((index % tiles) * tile, tile)
            rows = pl.ds(start, tile)
            q = q_ref[h, rows, :]
            lane = lax.broadcasted_iota(jnp.int32, (tile, wide), 1)
            for m in range(2):
                pick = (lane < HEAD) if m == 0 else (lane >= HEAD)
                q_map = jnp.where(pick, q, jnp.zeros_like(q))
                scores = lax.dot_general(q_map, block[h, :, :wide], NT, preferred_element_type=F32)
                if s == 0:
                    row = start + lax.broadcasted_iota(jnp.int32, scores.shape, 0)
                    col = lax.broadcasted_iota(jnp.int32, scores.shape, 1)
                    scores = jnp.where(col <= row, scores, -1e30)
                    fresh = jnp.max(scores, axis=1, keepdims=True)
                else:
                    top = top_ref[m, h, rows, :]
                    fresh = jnp.maximum(top, jnp.max(scores, axis=1, keepdims=True))
                expo = jnp.exp(scores - fresh)
                total = jnp.sum(expo, axis=1, keepdims=True)
                value = jnp.dot(
                    expo.astype(BF16), block[h, :, wide:], preferred_element_type=F32
                )
                if s:
                    shrink = jnp.exp(top - fresh)
                    total = total + sum_ref[m, h, rows, :] * shrink
                    value = value + val_ref[m, h, rows, :] * shrink
                top_ref[m, h, rows, :] = fresh
                sum_ref[m, h, rows, :] = total
                val_ref[m, h, rows, :] = value
            return carry

        lax.fori_loop(0, heads * tiles, one, 0)

    def attend_later(s):
        @pl.when(me >= s)
        def _():
            kv_copy(s).wait_recv()
            attend(s)

    attend(0)

    for s in range(ep):
        place_ref[s] = place_of(0, s)
        column = jnp.sum(jnp.where(row_at == col_at, route[s : s + 1, :], 0.0), axis=1, keepdims=True)
        route_ref[:, s : s + 1] = column

    @pl.when(has_guest)
    def _():
        for copy in guest_copies():
            copy.wait_recv()
        dispatch(1)

    pl.when(inner)(send_kv)

    m_tile = half // 2

    def hidden_of(src, first, count):
        def one(t, carry):
            rows = pl.ds(pl.multiple_of(t * m_tile, m_tile), m_tile)
            product = jnp.dot(rows_x[rows, :], w_gu[src], preferred_element_type=F32)
            for i in range(2):
                gate = product[:, i * lanes : i * lanes + unit]
                value = gate / (1.0 + jnp.exp(-gate)) * product[:, i * lanes + unit : (i + 1) * lanes]
                if subs == 1:
                    hid[src, 0, rows, i * unit : (i + 1) * unit] = value.astype(BF16)
                else:
                    hid[src, i, rows, :] = value.astype(BF16)
            return carry

        lax.fori_loop(first, first + count, one, 0)

    def h_copy(src):
        return remote(
            hid.at[src, :, pl.ds(half, half)],
            hid.at[src, :, pl.ds(0, half)],
            h_s.at[src],
            h_r.at[src],
            {"tp": (z - inward) * 2 + core},
        )

    @pl.when(inner)
    def _():
        for s in range(1, ep):
            x_copy(0, s).wait_recv()
        ready_gu(z)
        hidden_of(z, 0, 2)

    pass_gu(1, True)

    @pl.when(inner)
    def _():
        ready_gu(z + inward)
        hidden_of(z + inward, 0, 2)

    pass_gu(1, False)
    for c in range(CHUNKS):
        pass_dn(1, True, c)

    @pl.when(has_guest)
    def _():
        for s in range(1, ep):
            x_copy(1, s).wait_recv()
        hidden_of(z, 2, 2)
        h_copy(z).start()
        hidden_of(z + inward, 2, 2)
        h_copy(z + inward).start()

    def use_gu(src):
        ready_gu(src)
        hidden_of(src, 0, 2)

        @pl.when(has_guest)
        def _():
            hidden_of(src, 2, 2)
            h_copy(src).start()

    pl.when(inner)(lambda: use_gu(z - inward))
    early = 1 + (ep - 1) // 3
    later = 1 + 2 * (ep - 1) // 3
    for s in range(1, early):
        attend_later(s)
    for c in range(CHUNKS):
        pass_dn(1, False, c)
    for s in range(early, later):
        attend_later(s)
    for k in range(2, chips):
        for near in (True, False):
            pass_gu(k, near)
            far = source(k, near)[0]
            pl.when(inner & on_line(far))(lambda far=far: use_gu(far))
    for s in range(later, ep):
        attend_later(s)

    def finish(index, carry):
        h = index // tiles
        rows = pl.ds(pl.multiple_of((index % tiles) * tile, tile), tile)
        diff = val_ref[0, h, rows, :] / sum_ref[0, h, rows, :] - mix_ref[h] * (
            val_ref[1, h, rows, :] / sum_ref[1, h, rows, :]
        )
        scaled = diff * lax.rsqrt(jnp.mean(diff * diff, axis=1, keepdims=True) + 1e-05)
        att[h, rows, :] = (scaled * gain_ref[...]).astype(BF16)
        return carry

    lax.fori_loop(0, heads * tiles, finish, 0)

    block = length // tp

    def project(t, carry):
        rows = pl.ds(pl.multiple_of(t * 2 * block, 2 * block), 2 * block)
        total = 0.0
        for h in range(heads):
            total = total + jnp.dot(att[h, rows, :], ow_ref[h], preferred_element_type=F32)
        part[0, t] = total[:block].astype(BF16)
        part[1, t] = total[block:].astype(BF16)
        return carry

    lax.fori_loop(0, chips, project, 0)
    pair_copy = remote(part.at[1 - core], pair, pr_s, pr_r, {"tp": other})
    pair_copy.start()
    pair_copy.wait_recv()

    def add_pair(t, carry):
        chip_sum[t] = (part[core, t].astype(F32) + pair[t].astype(F32)).astype(BF16)
        return carry

    lax.fori_loop(0, chips, add_pair, 0)

    def line_copy(side, t, first):
        return remote(
            chip_sum.at[t] if first else line_out.at[side, t],
            landed.at[side, t],
            rs_s.at[side, t],
            rs_r.at[side, t],
            {"tp": (z + 1 - 2 * side) * 2 + core},
        )

    def stage_each(k, do):
        for side in range(2):
            at = k if side == 0 else chips - 1 - k
            targets = range(chips - 1, k, -1) if side == 0 else range(chips - 1 - k)

            @pl.when(z == at)
            def _(side=side, targets=targets):
                for t in targets:
                    do(side, t, k == 0)

    def stage_send(side, t, first):
        copy = line_copy(side, t, first)
        if not first:
            copy.wait_recv()
            line_out[side, t] = (
                chip_sum[t].astype(F32) + landed[side, t].astype(F32)
            ).astype(BF16)
        copy.start()

    stage_each(0, stage_send)
    if chips > 2:
        stage_each(1, stage_send)

    @pl.when(is_end)
    def _():
        for src in range(chips):
            h_copy(src).wait_recv()

    def back_copy(c, s):
        return remote(
            back.at[c, pl.ds(s * cap, cap)],
            ret.at[c, s],
            b_s.at[c, s],
            b_r.at[c, s],
            {"ep": lax.rem(me + ep - s, ep)},
        )

    def down_of(c):
        def one(t, carry):
            rows = pl.ds(pl.multiple_of(t * m_tile, m_tile), m_tile)
            total = 0.0
            for src in range(chips):
                for i in range(subs):
                    total = total + lax.dot_general(
                        hid[src, i, rows, :], w_dn[src, i, c], NT, preferred_element_type=F32
                    )
            back[c, rows, :] = total.astype(BF16)
            return carry

        lax.fori_loop(0, 2, one, 0)

    def combine(c):
        total = 0.0
        for s in range(ep):
            if s == 0:
                block_rows = back[c, :cap, :]
            else:
                back_copy(c, s).wait_recv()
                block_rows = ret[c, s]
            picked = lax.dot_general(place_ref[s], block_rows, TN, preferred_element_type=F32)
            total = total + route_ref[:, s : s + 1] * picked
        routed_ref[:, c * step : (c + 1) * step] = total.astype(BF16)

    for c in range(CHUNKS):
        for k in range(2, chips):
            for near in (True, False):
                pass_dn(k, near, c)
        for src in range(chips):
            sd_copy(src, c).wait_recv()
        down_of(c)
        for s in range(1, ep):
            back_copy(c, s).start()
        if c == 1:
            for k in range(2, chips - 1):
                stage_each(k, stage_send)
        if c > 1:
            combine(c - 2)

    mixed_ref[...] = chip_sum[z]
    for side in range(2):

        @pl.when((z > 0) if side == 0 else (z < chips - 1))
        def _(side=side):
            line_copy(side, z, False).wait_recv()
            mixed_ref[...] = (
                mixed_ref[...].astype(F32) + landed[side, z].astype(F32)
            ).astype(BF16)

    for c in range(max(CHUNKS - 2, 0), CHUNKS):
        combine(c)

    for s in range(1, ep):
        pl.when(me + s < ep)(lambda s=s: kv_copy(s).wait_send())

        @pl.when(inner)
        def _(s=s):
            x_copy(0, s).wait_send()

        @pl.when(has_guest)
        def _(s=s):
            x_copy(1, s).wait_send()

    @pl.when(is_end)
    def _():
        for copy in guest_copies():
            copy.wait_send()

    @pl.when(has_guest)
    def _():
        for src in range(chips):
            h_copy(src).wait_send()

    for k in range(chips):
        for near in (True, False):
            src, way = source(k, near)

            @pl.when(on_line(src))
            def _(k=k, near=near, src=src, way=way):
                @pl.when(wants_gu(z + way) & (inner | (k == 0)))
                def _():
                    for j in range(PIECES):
                        gu_copy(src, j, way).wait_send()

                @pl.when(on_line(z + way))
                def _():
                    for c in range(CHUNKS):
                        dn_copy(src, c, way).wait_send()

                if k or near:

                    @pl.when(inner)
                    def _():
                        for j in range(PIECES):
                            sg_copy(src, j).wait_send()

                    for c in range(CHUNKS):
                        sd_copy(src, c).wait_send()

    pair_copy.wait_send()
    for k in range(chips - 1):
        stage_each(k, lambda side, t, first: line_copy(side, t, first).wait_send())
    for c in range(CHUNKS):
        for s in range(1, ep):
            back_copy(c, s).wait_send()


def per_device(
    queries,
    keys,
    values,
    mixing,
    head_gain,
    out_weight,
    tokens_b,
    norm_gain,
    expert_ids,
    group_gate,
    expert_gate,
    gate_weight,
    up_weight,
    down_weight,
):
    ep = lax.axis_size("ep")
    tp = lax.axis_size("tp")
    chips = tp // 2
    length, heads, wide = queries.shape
    val = values.shape[2]
    local_rows, width = tokens_b.shape
    top_count = expert_ids.shape[1]
    unit = gate_weight.shape[2]
    assert gate_weight.shape[0] == 1 and wide == 2 * HEAD and chips >= 4 and ep <= RANKS
    capacity = 3 * local_rows * top_count // (2 * ep)
    cap = -(-capacity // 16) * 16
    step = width // CHUNKS

    scaled = (queries.astype(F32) * (1.0 / math.sqrt(HEAD))).astype(BF16).transpose(1, 0, 2)
    kv = jnp.concatenate([keys, values], axis=2).transpose(1, 0, 2)
    gate, up = gate_weight[0], up_weight[0]
    subs = 1
    if unit % 128:
        gate = jnp.concatenate([gate, up], axis=1)
        subs = 2
    half = ep * cap
    block = length // tp
    vmem = pl.BlockSpec(memory_space=pltpu.VMEM)
    anywhere = pl.BlockSpec(memory_space=pl.ANY)
    dma = pltpu.SemaphoreType.DMA
    return pl.pallas_call(
        functools.partial(kernel, ep, tp),
        out_shape=(
            jax.ShapeDtypeStruct((block, width), BF16),
            jax.ShapeDtypeStruct((local_rows, width), BF16),
        ),
        in_specs=[pl.BlockSpec(memory_space=pltpu.SMEM)] + [vmem] * 9 + [anywhere] * 3,
        out_specs=(vmem, vmem),
        scratch_shapes=[
            pltpu.VMEM((ep, heads, length, wide + val), BF16),
            pltpu.VMEM((chips, width, 4 * unit), BF16),
            pltpu.VMEM((chips, subs, CHUNKS, step, 2 * unit // subs), BF16),
            pltpu.VMEM((2 * half, width), BF16),
            pltpu.VMEM((2, ep - 1, cap, width), BF16),
            pltpu.VMEM((2, local_rows, width), BF16),
            pltpu.VMEM((2, RANKS, local_rows), F32),
            pltpu.VMEM((chips, subs, 2 * half, 2 * unit // subs), BF16),
            pltpu.VMEM((CHUNKS, half, step), BF16),
            pltpu.VMEM((CHUNKS, ep, cap, step), BF16),
            pltpu.VMEM((2, heads, length, 1), F32),
            pltpu.VMEM((2, heads, length, 1), F32),
            pltpu.VMEM((2, heads, length, val), F32),
            pltpu.VMEM((heads, length, val), BF16),
            pltpu.VMEM((2, chips, block, width), BF16),
            pltpu.VMEM((chips, block, width), BF16),
            pltpu.VMEM((chips, block, width), BF16),
            pltpu.VMEM((2, chips, block, width), BF16),
            pltpu.VMEM((2, chips, block, width), BF16),
            pltpu.VMEM((ep, cap, local_rows), BF16),
            pltpu.VMEM((local_rows, ep), F32),
            dma((3,)),
            dma((ep,)),
            dma((ep,)),
            dma((2,)),
            dma((2,)),
            dma((2, ep)),
            dma((2, ep)),
            dma((2, chips, PIECES)),
            dma((chips, PIECES)),
            dma((chips, PIECES)),
            dma((chips, PIECES)),
            dma((2, chips, CHUNKS)),
            dma((chips, CHUNKS)),
            dma((chips, CHUNKS)),
            dma((chips, CHUNKS)),
            dma((chips,)),
            dma((chips,)),
            dma,
            dma,
            dma((2, chips)),
            dma((2, chips)),
            dma((CHUNKS, ep)),
            dma((CHUNKS, ep)),
        ],
        compiler_params=pltpu.CompilerParams(
            collective_id=0, has_side_effects=True, vmem_limit_bytes=62 * 1024 * 1024
        ),
    )(
        mixing,
        scaled,
        kv,
        head_gain[None],
        out_weight,
        tokens_b,
        norm_gain[None],
        expert_ids.T,
        group_gate[None],
        expert_gate.T,
        gate,
        up,
        down_weight[0].reshape(CHUNKS, step, unit),
    )


def solution(mesh):
    placed = (
        P("ep", "tp", None),
        P("ep", "tp", None),
        P("ep", "tp", None),
        P("tp"),
        P(),
        P("tp", None, None),
        P(("ep", "tp"), None),
        P(),
        P(("ep", "tp"), None),
        P(("ep", "tp")),
        P(("ep", "tp"), None),
        P("ep", None, "tp"),
        P("ep", None, "tp"),
        P("ep", None, "tp"),
    )
    return jax.shard_map(
        per_device,
        mesh=mesh,
        in_specs=placed,
        out_specs=(P(("ep", "tp"), None), P(("ep", "tp"), None)),
        check_vma=False,
    )
```

```python
import functools
import math

import jax
import jax.numpy as jnp
from jax import lax
from jax.experimental import pallas as pl
from jax.experimental.pallas import tpu as pltpu
from jax.sharding import PartitionSpec as P

HEAD = 64
CHUNKS = 4
QUARTER = CHUNKS // 4
PIECES = 2
RANKS = 16
F32 = jnp.float32
BF16 = jnp.bfloat16
MESH = pl.DeviceIdType.MESH
NT = (((1,), (1,)), ((), ()))
TN = (((0,), (0,)), ((), ()))


def kernel(
    ep,
    tp,
    mix_ref,
    gain_ref,
    norm_ref,
    ids_ref,
    group_ref,
    gates_ref,
    q_in,
    k_in,
    v_in,
    ow_in,
    tok_in,
    gate_ref,
    up_ref,
    dn_ref,
    mixed_ref,
    routed_ref,
    q_raw,
    k_raw,
    v_raw,
    ow_ref,
    tok_ref,
    q_ref,
    kv_all,
    w_gu,
    w_dn,
    rows_x,
    out_ref,
    nrm,
    rank_ref,
    hid,
    back,
    ret,
    top_ref,
    sum_ref,
    val_ref,
    att,
    part,
    pair,
    chip_sum,
    landed,
    line_out,
    place_ref,
    route_ref,
    local_sem,
    kv_s,
    kv_r,
    t_s,
    t_r,
    x_s,
    x_r,
    gu_s,
    gu_r,
    sg_s,
    sg_r,
    dn_s,
    dn_r,
    sd_s,
    sd_r,
    h_s,
    h_r,
    pr_s,
    pr_r,
    rs_s,
    rs_r,
    b_s,
    b_r,
):
    chips = tp // 2
    me = lax.axis_index("ep")
    mine = lax.axis_index("tp")
    z = mine // 2
    core = mine % 2
    other = z * 2 + 1 - core
    inward = 1 - 2 * (z // (chips // 2))
    heads, length, wide = q_ref.shape
    val = val_ref.shape[3]
    local_rows, width = tok_ref.shape
    half = rows_x.shape[0] // 2
    cap = half // ep
    step = w_dn.shape[3]
    lanes = w_gu.shape[2] // 2
    unit = lanes // 2
    subs = w_dn.shape[1]
    deep = width // PIECES
    joined = gate_ref.shape[1] != unit
    inner = (z >= 1) & (z <= chips - 2)
    is_end = (z == 0) | (z == chips - 1)
    has_guest = (z == 1) | (z == chips - 2)

    def remote(src, dst, send, recv, target):
        return pltpu.make_async_remote_copy(
            src_ref=src,
            dst_ref=dst,
            send_sem=send,
            recv_sem=recv,
            device_id=target,
            device_id_type=MESH,
        )

    if joined:
        own_gu = [pltpu.make_async_copy(gate_ref, w_gu.at[z, :, pl.ds(0, lanes)], local_sem.at[0])]
    else:
        own_gu = [
            pltpu.make_async_copy(gate_ref, w_gu.at[z, :, pl.ds(0, unit)], local_sem.at[0]),
            pltpu.make_async_copy(up_ref, w_gu.at[z, :, pl.ds(unit, unit)], local_sem.at[1]),
        ]
    if subs == 1:
        own_dn = pltpu.make_async_copy(dn_ref, w_dn.at[z, 0, :, :, pl.ds(0, unit)], local_sem.at[2])
    else:
        own_dn = pltpu.make_async_copy(dn_ref, w_dn.at[z, 0], local_sem.at[2])
    own_kv = [
        pltpu.make_async_copy(k_in, k_raw, local_sem.at[3]),
        pltpu.make_async_copy(v_in, v_raw, local_sem.at[4]),
        pltpu.make_async_copy(q_in, q_raw, local_sem.at[5]),
    ]
    own_tok = pltpu.make_async_copy(tok_in, tok_ref, local_sem.at[6])
    own_ow = pltpu.make_async_copy(ow_in, ow_ref, local_sem.at[7])

    barrier = pltpu.get_barrier_semaphore()
    for s in range(1, ep):
        pl.semaphore_signal(
            barrier, inc=1, device_id={"ep": (me + s) % ep}, device_id_type=MESH
        )
    for s in range(1, tp):
        pl.semaphore_signal(
            barrier, inc=1, device_id={"tp": (mine + s) % tp}, device_id_type=MESH
        )
    for copy in [own_tok] + own_gu + own_kv + [own_dn, own_ow]:
        copy.start()
    pl.semaphore_wait(barrier, ep + tp - 2)

    def on_line(at):
        return (at >= 0) & (at <= chips - 1)

    def wants_gu(at):
        return (at >= 1) & (at <= chips - 2)

    def gu_part(src, j):
        return w_gu.at[src, pl.ds(j * deep, deep), pl.ds(0, lanes)]

    def gu_copy(src, j, way):
        return remote(
            gu_part(src, j),
            gu_part(src, j),
            gu_s.at[(1 - way) // 2, src, j],
            gu_r.at[src, j],
            {"tp": (z + way) * 2 + core},
        )

    def sg_copy(src, j):
        return remote(
            gu_part(src, j),
            w_gu.at[src, pl.ds(j * deep, deep), pl.ds(lanes, lanes)],
            sg_s.at[src, j],
            sg_r.at[src, j],
            {"tp": other},
        )

    def dn_part(src, c, which):
        if subs == 1:
            return w_dn.at[src, 0, c, :, pl.ds(which * unit, unit)]
        return w_dn.at[src, which, c]

    def dn_copy(src, c, way):
        return remote(
            dn_part(src, c, 0),
            dn_part(src, c, 0),
            dn_s.at[(1 - way) // 2, src, c],
            dn_r.at[src, c],
            {"tp": (z + way) * 2 + core},
        )

    def sd_copy(src, c):
        return remote(
            dn_part(src, c, 0), dn_part(src, c, 1), sd_s.at[src, c], sd_r.at[src, c], {"tp": other}
        )

    def start_own():
        for copy in own_gu:
            copy.wait()
        for way in (inward, -inward):

            @pl.when(wants_gu(z + way))
            def _(way=way):
                for j in range(PIECES):
                    gu_copy(z, j, way).start()

        @pl.when(inner)
        def _():
            for j in range(PIECES):
                sg_copy(z, j).start()

        own_dn.wait()

        @pl.when(is_end)
        def _():
            for c in range(CHUNKS):
                dn_copy(z, c, inward).start()

        @pl.when(inner)
        def _():
            for c in range(CHUNKS):
                dn_copy(z, c, -inward).start()
            for c in range(2 * QUARTER, CHUNKS):
                dn_copy(z, c, inward).start()

        for c in range(CHUNKS):
            sd_copy(z, c).start()

    def source(k, near):
        return (z + k * inward, -inward) if near else (z - k * inward, inward)

    def pass_gu(k, near, j):
        src, way = source(k, near)

        @pl.when(inner & on_line(src))
        def _():
            gu_copy(src, j, way).wait_recv()
            pl.when(wants_gu(z + way))(lambda: gu_copy(src, j, way).start())
            sg_copy(src, j).start()

    def ready_gu(src):
        for j in range(PIECES):
            sg_copy(src, j).wait_recv()

    def pass_dn(k, near, c):
        src, way = source(k, near)

        @pl.when(on_line(src))
        def _():
            dn_copy(src, c, way).wait_recv()
            pl.when(on_line(z + way))(lambda: dn_copy(src, c, way).start())
            sd_copy(src, c).start()

    square_plane = ep == 4
    mid_rows = length // 2

    def kv_move(src, dst, sem, target):
        return remote(src, dst, kv_s.at[sem], kv_r.at[sem], {"ep": target})

    def kv_copy(s):
        return kv_move(kv_all.at[0], kv_all.at[s], s, lax.rem(me + s, ep))

    def kv_half(s, i):
        rows = pl.ds(i * mid_rows, mid_rows)
        return kv_move(kv_all.at[s, :, rows], kv_all.at[3, :, rows], 3 + i, 3)

    def kv_corner():
        return kv_move(kv_all.at[2], kv_all.at[1], 1, 2)

    if square_plane:
        near_sends = [((me == 0) | (me == 2), 1), (me <= 1, 2)]
        far_sends = [
            (me == 1, lambda: kv_half(1, 0)),
            (me == 2, lambda: kv_half(2, 1)),
            (me == 3, kv_corner),
        ]
        early_blocks = [((me == 1) | (me == 3), 1), (me >= 2, 2)]
        late_blocks = [(me >= 2, jnp.where(me == 2, 1, 3))]
    else:
        near_sends = [(me + s < ep, s) for s in range(1, ep - 1)]
        far_sends = [(me + ep - 1 < ep, lambda: kv_copy(ep - 1))]
        early_blocks = [(me >= s, s) for s in range(1, ep - 1)]
        late_blocks = [(me >= ep - 1, ep - 1)]

    def send_near():
        for sends, s in near_sends:
            pl.when(sends)(lambda s=s: kv_copy(s).start())

    def receive_near():
        for has, s in early_blocks:
            pl.when(has)(lambda s=s: kv_copy(s).wait_recv())

    def send_far():
        for sends, copy in far_sends:
            pl.when(sends)(lambda copy=copy: copy().start())

    def receive_far():
        if square_plane:
            pl.when(me == 2)(lambda: kv_corner().wait_recv())

            @pl.when(me == 3)
            def _():
                kv_half(1, 0).wait_recv()
                kv_half(2, 1).wait_recv()

        else:
            pl.when(me >= ep - 1)(lambda: kv_copy(ep - 1).wait_recv())

    pl.when(inner)(start_own)
    own_tok.wait()

    relative = ids_ref[...] - me
    relative = jnp.where(relative < 0, relative + ep, relative)
    table = (RANKS, local_rows)
    expert_row = lax.broadcasted_iota(jnp.int32, table, 0)
    named = jnp.zeros(table, F32)
    route = jnp.zeros(table, F32)
    for k in range(ids_ref.shape[0]):
        hit = expert_row == relative[k : k + 1, :]
        named = jnp.where(hit, 1.0, named)
        route = route + jnp.where(hit, group_ref[...] * gates_ref[k : k + 1, :], 0.0)
    square = (local_rows, local_rows)
    row_at = lax.broadcasted_iota(jnp.int32, square, 0)
    col_at = lax.broadcasted_iota(jnp.int32, square, 1)
    before = jnp.where(row_at < col_at, 1.0, 0.0).astype(BF16)
    rank = jnp.dot(named.astype(BF16), before, preferred_element_type=F32)
    rank_ref[0] = jnp.where(named > 0.5, rank, -1.0)
    tokens = tok_ref[...].astype(F32)
    nrm[0] = (
        tokens
        * lax.rsqrt(jnp.mean(tokens * tokens, axis=1, keepdims=True) + 1e-06)
        * norm_ref[...]
    ).astype(BF16)

    def guest_copies():
        target = {"tp": (z + inward) * 2 + core}
        return (
            remote(nrm.at[0], nrm.at[1], t_s.at[0], t_r.at[0], target),
            remote(rank_ref.at[0], rank_ref.at[1], t_s.at[1], t_r.at[1], target),
        )

    @pl.when(is_end)
    def _():
        for copy in guest_copies():
            copy.start()
        start_own()

    for copy in own_kv:
        copy.wait()
    part_rows = min(128, length)

    def lay_kv(t, carry):
        rows = pl.ds(pl.multiple_of(t * part_rows, part_rows), part_rows)
        k_flat = k_raw[rows].reshape(part_rows, heads * wide)
        v_flat = v_raw[rows].reshape(part_rows, heads * val)
        for h in range(heads):
            kv_all[0, h, rows, :wide] = k_flat[:, h * wide : (h + 1) * wide]
            kv_all[0, h, rows, wide:] = v_flat[:, h * val : (h + 1) * val]
        return carry

    def lay_q(t, carry):
        rows = pl.ds(pl.multiple_of(t * part_rows, part_rows), part_rows)
        q_flat = q_raw[rows].reshape(part_rows, heads * wide)
        for h in range(heads):
            q = q_flat[:, h * wide : (h + 1) * wide].astype(F32) * (1.0 / math.sqrt(HEAD))
            q_ref[h, rows, :] = q.astype(BF16)
        return carry

    lax.fori_loop(0, length // part_rows, lay_kv, 0)
    send_near()
    lax.fori_loop(0, length // part_rows, lay_q, 0)

    def x_copy(g, s):
        return remote(
            out_ref.at[g, s - 1],
            rows_x.at[pl.ds(g * half + s * cap, cap)],
            x_s.at[g, s],
            x_r.at[g, s],
            {"ep": lax.rem(me + s, ep)},
        )

    slot_row = lax.broadcasted_iota(jnp.int32, (cap, local_rows), 0).astype(F32)

    def place_of(g, s):
        return jnp.where(rank_ref[g, s : s + 1, :] == slot_row, 1.0, 0.0).astype(BF16)

    def dispatch(g):
        for s in list(range(1, ep)) + [0]:
            place = place_of(g, s)
            for n in range(CHUNKS):
                cols = slice(n * step, (n + 1) * step)
                picked = jnp.dot(place, nrm[g, :, cols], preferred_element_type=F32).astype(BF16)
                if s:
                    out_ref[g, s - 1, :, cols] = picked
                else:
                    rows_x[g * half : g * half + cap, cols] = picked
            if s:
                x_copy(g, s).start()

    tile = min(256, length)
    tiles = length // tile

    def attend(s, first=False):
        block = kv_all.at[s]

        def one(index, carry):
            h = index // tiles
            start = pl.multiple_of((index % tiles) * tile, tile)
            rows = pl.ds(start, tile)
            q = q_ref[h, rows, :]
            lane = lax.broadcasted_iota(jnp.int32, (tile, wide), 1)
            for m in range(2):
                pick = (lane < HEAD) if m == 0 else (lane >= HEAD)
                q_map = jnp.where(pick, q, jnp.zeros_like(q))
                scores = lax.dot_general(q_map, block[h, :, :wide], NT, preferred_element_type=F32)
                if first:
                    row = start + lax.broadcasted_iota(jnp.int32, scores.shape, 0)
                    col = lax.broadcasted_iota(jnp.int32, scores.shape, 1)
                    scores = jnp.where(col <= row, scores, -1e30)
                    fresh = jnp.max(scores, axis=1, keepdims=True)
                else:
                    top = top_ref[m, h, rows, :]
                    fresh = jnp.maximum(top, jnp.max(scores, axis=1, keepdims=True))
                expo = jnp.exp(scores - fresh)
                total = jnp.sum(expo, axis=1, keepdims=True)
                value = jnp.dot(
                    expo.astype(BF16), block[h, :, wide:], preferred_element_type=F32
                )
                if not first:
                    shrink = jnp.exp(top - fresh)
                    total = total + sum_ref[m, h, rows, :] * shrink
                    value = value + val_ref[m, h, rows, :] * shrink
                top_ref[m, h, rows, :] = fresh
                sum_ref[m, h, rows, :] = total
                val_ref[m, h, rows, :] = value
            return carry

        lax.fori_loop(0, heads * tiles, one, 0)

    attend(0, True)

    for s in range(ep):
        place_ref[s] = place_of(0, s)
        column = jnp.sum(jnp.where(row_at == col_at, route[s : s + 1, :], 0.0), axis=1, keepdims=True)
        route_ref[:, s : s + 1] = column

    m_tile = half // 2

    def hidden_of(src, first, count):
        def one(t, carry):
            rows = pl.ds(pl.multiple_of(t * m_tile, m_tile), m_tile)
            product = jnp.dot(rows_x[rows, :], w_gu[src], preferred_element_type=F32)
            for i in range(2):
                gate = product[:, i * lanes : i * lanes + unit]
                value = gate / (1.0 + jnp.exp(-gate)) * product[:, i * lanes + unit : (i + 1) * lanes]
                if subs == 1:
                    hid[src, 0, rows, i * unit : (i + 1) * unit] = value.astype(BF16)
                else:
                    hid[src, i, rows, :] = value.astype(BF16)
            return carry

        lax.fori_loop(first, first + count, one, 0)

    def h_copy(src):
        return remote(
            hid.at[src, :, pl.ds(half, half)],
            hid.at[src, :, pl.ds(0, half)],
            h_s.at[src],
            h_r.at[src],
            {"tp": (z - inward) * 2 + core},
        )

    @pl.when(has_guest)
    def _():
        for copy in guest_copies():
            copy.wait_recv()
        dispatch(1)

    receive_near()
    send_far()
    pl.when(inner)(lambda: dispatch(0))
    for has, s in early_blocks:
        pl.when(has)(lambda s=s: attend(s))
    for j in range(PIECES):
        pass_gu(1, True, j)
    for j in range(PIECES - 1):
        pass_gu(1, False, j)

    def pass_near(first, last):
        for c in range(first * QUARTER, last * QUARTER):
            pass_dn(1, True, c)

    pass_near(2, 4)

    @pl.when(inner)
    def _():
        ready_gu(z)
        ready_gu(z + inward)

    def guest_hidden(src):
        hidden_of(src, 2, 2)
        h_copy(src).start()

    @pl.when(has_guest)
    def _():
        for s in range(1, ep):
            x_copy(1, s).wait_recv()
        guest_hidden(z)
        guest_hidden(z + inward)

    pass_gu(1, False, PIECES - 1)

    @pl.when(inner)
    def _():
        for c in range(QUARTER):
            dn_copy(z, c, inward).start()
        ready_gu(z - inward)
        pl.when(has_guest)(lambda: guest_hidden(z - inward))

    for c in range(2 * QUARTER):
        if c >= QUARTER:
            pl.when(inner)(lambda c=c: dn_copy(z, c, inward).start())
        pass_dn(1, False, c)

    receive_far()
    for has, s in late_blocks:
        pl.when(has)(lambda s=s: attend(s))

    def finish(index, carry):
        h = index // tiles
        rows = pl.ds(pl.multiple_of((index % tiles) * tile, tile), tile)
        diff = val_ref[0, h, rows, :] / sum_ref[0, h, rows, :] - mix_ref[h] * (
            val_ref[1, h, rows, :] / sum_ref[1, h, rows, :]
        )
        scaled = diff * lax.rsqrt(jnp.mean(diff * diff, axis=1, keepdims=True) + 1e-05)
        att[h, rows, :] = (scaled * gain_ref[...]).astype(BF16)
        return carry

    lax.fori_loop(0, heads * tiles, finish, 0)

    block = length // tp

    def project(t, carry):
        rows = pl.ds(pl.multiple_of(t * 2 * block, 2 * block), 2 * block)
        total = 0.0
        for h in range(heads):
            total = total + jnp.dot(att[h, rows, :], ow_ref[h], preferred_element_type=F32)
        part[0, t] = total[:block].astype(BF16)
        part[1, t] = total[block:].astype(BF16)
        return carry

    own_ow.wait()
    lax.fori_loop(0, chips, project, 0)
    pair_copy = remote(part.at[1 - core], pair, pr_s, pr_r, {"tp": other})
    pair_copy.start()
    pair_copy.wait_recv()

    def add_pair(t, carry):
        chip_sum[t] = (part[core, t].astype(F32) + pair[t].astype(F32)).astype(BF16)
        return carry

    lax.fori_loop(0, chips, add_pair, 0)

    def line_copy(side, t, first):
        return remote(
            chip_sum.at[t] if first else line_out.at[side, t],
            landed.at[side, t],
            rs_s.at[side, t],
            rs_r.at[side, t],
            {"tp": (z + 1 - 2 * side) * 2 + core},
        )

    def stage_each(k, do):
        for side in range(2):
            at = k if side == 0 else chips - 1 - k
            targets = range(chips - 1, k, -1) if side == 0 else range(chips - 1 - k)

            @pl.when(z == at)
            def _(side=side, targets=targets):
                for t in targets:
                    do(side, t, k == 0)

    def stage_send(side, t, first):
        copy = line_copy(side, t, first)
        if not first:
            copy.wait_recv()
            line_out[side, t] = (
                chip_sum[t].astype(F32) + landed[side, t].astype(F32)
            ).astype(BF16)
        copy.start()

    stage_each(0, stage_send)

    for c in range(2 * QUARTER, CHUNKS):
        pass_dn(1, False, c)
    for k in range(2, chips):
        for near in (True, False):
            for j in range(PIECES):
                pass_gu(k, near, j)
            far = source(k, near)[0]

            @pl.when(inner & on_line(far))
            def _(far=far):
                ready_gu(far)
                pl.when(has_guest)(lambda: guest_hidden(far))

    def back_copy(c, s):
        return remote(
            back.at[c, pl.ds(s * cap, cap)],
            ret.at[c, s],
            b_s.at[c, s],
            b_r.at[c, s],
            {"ep": lax.rem(me + ep - s, ep)},
        )

    def down_of(c):
        def one(t, carry):
            rows = pl.ds(pl.multiple_of(t * m_tile, m_tile), m_tile)
            total = 0.0
            for src in range(chips):
                for i in range(subs):
                    total = total + lax.dot_general(
                        hid[src, i, rows, :], w_dn[src, i, c], NT, preferred_element_type=F32
                    )
            back[c, rows, :] = total.astype(BF16)
            return carry

        lax.fori_loop(0, 2, one, 0)

    def combine(c):
        total = 0.0
        for s in range(ep):
            if s == 0:
                block_rows = back[c, :cap, :]
            else:
                back_copy(c, s).wait_recv()
                block_rows = ret[c, s]
            picked = lax.dot_general(place_ref[s], block_rows, TN, preferred_element_type=F32)
            total = total + route_ref[:, s : s + 1] * picked
        routed_ref[:, c * step : (c + 1) * step] = total.astype(BF16)

    def pass_far(c):
        for k in range(2, chips):
            for near in (True, False):
                pass_dn(k, near, c)

    def give_back(c):
        for src in range(chips):
            sd_copy(src, c).wait_recv()
        down_of(c)
        for s in range(1, ep):
            back_copy(c, s).start()

    def own_hidden(first, last):
        lax.fori_loop(first, last, lambda src, carry: (hidden_of(src, 0, 2), carry)[1], 0)

    @pl.when(inner)
    def _():
        pass_near(0, 1)
        for s in range(1, ep):
            x_copy(0, s).wait_recv()
        own_hidden(0, chips // 2)
        for c in range(QUARTER):
            pass_far(c)
        own_hidden(chips // 2, chips)
        pass_near(1, 2)
        for c in range(QUARTER):
            give_back(c)
        for c in range(QUARTER, 2 * QUARTER):
            pass_far(c)
            give_back(c)
        stage_each(1, stage_send)
        for c in range(2 * QUARTER, CHUNKS):
            pass_far(c)
            give_back(c)

    @pl.when(is_end)
    def _():
        pass_near(0, 1)
        for c in range(QUARTER):
            pass_far(c)
        for src in range(chips):
            h_copy(src).wait_recv()
        for c in range(QUARTER):
            give_back(c)
        pass_near(1, 2)
        for c in range(QUARTER, CHUNKS):
            pass_far(c)
            give_back(c)

    for c in range(CHUNKS):
        if c == CHUNKS // 2:
            for k in range(2, chips - 1):
                stage_each(k, stage_send)
        combine(c)

    mixed_ref[...] = chip_sum[z]
    for side in range(2):

        @pl.when((z > 0) if side == 0 else (z < chips - 1))
        def _(side=side):
            line_copy(side, z, False).wait_recv()
            mixed_ref[...] = (
                mixed_ref[...].astype(F32) + landed[side, z].astype(F32)
            ).astype(BF16)

    for sends, s in near_sends:
        pl.when(sends)(lambda s=s: kv_copy(s).wait_send())
    for sends, copy in far_sends:
        pl.when(sends)(lambda copy=copy: copy().wait_send())
    for s in range(1, ep):

        @pl.when(inner)
        def _(s=s):
            x_copy(0, s).wait_send()

        @pl.when(has_guest)
        def _(s=s):
            x_copy(1, s).wait_send()

    @pl.when(is_end)
    def _():
        for copy in guest_copies():
            copy.wait_send()

    @pl.when(has_guest)
    def _():
        for src in range(chips):
            h_copy(src).wait_send()

    for k in range(chips):
        for near in (True, False):
            src, way = source(k, near)

            @pl.when(on_line(src))
            def _(k=k, near=near, src=src, way=way):
                @pl.when(wants_gu(z + way) & (inner | (k == 0)))
                def _():
                    for j in range(PIECES):
                        gu_copy(src, j, way).wait_send()

                @pl.when(on_line(z + way))
                def _():
                    for c in range(CHUNKS):
                        dn_copy(src, c, way).wait_send()

                if k or near:

                    @pl.when(inner)
                    def _():
                        for j in range(PIECES):
                            sg_copy(src, j).wait_send()

                    for c in range(CHUNKS):
                        sd_copy(src, c).wait_send()

    pair_copy.wait_send()
    for k in range(chips - 1):
        stage_each(k, lambda side, t, first: line_copy(side, t, first).wait_send())
    for c in range(CHUNKS):
        for s in range(1, ep):
            back_copy(c, s).wait_send()


def per_device(
    queries,
    keys,
    values,
    mixing,
    head_gain,
    out_weight,
    tokens_b,
    norm_gain,
    expert_ids,
    group_gate,
    expert_gate,
    gate_weight,
    up_weight,
    down_weight,
):
    ep = lax.axis_size("ep")
    tp = lax.axis_size("tp")
    chips = tp // 2
    length, heads, wide = queries.shape
    val = values.shape[2]
    local_rows, width = tokens_b.shape
    top_count = expert_ids.shape[1]
    unit = gate_weight.shape[2]
    assert gate_weight.shape[0] == 1 and wide == 2 * HEAD and chips >= 4 and ep <= RANKS
    capacity = 3 * local_rows * top_count // (2 * ep)
    cap = -(-capacity // 16) * 16
    step = width // CHUNKS

    gate, up = gate_weight[0], up_weight[0]
    subs = 1
    if unit % 128:
        gate = jnp.concatenate([gate, up], axis=1)
        subs = 2
    half = ep * cap
    block = length // tp
    vmem = pl.BlockSpec(memory_space=pltpu.VMEM)
    anywhere = pl.BlockSpec(memory_space=pl.ANY)
    dma = pltpu.SemaphoreType.DMA
    return pl.pallas_call(
        functools.partial(kernel, ep, tp),
        out_shape=(
            jax.ShapeDtypeStruct((block, width), BF16),
            jax.ShapeDtypeStruct((local_rows, width), BF16),
        ),
        in_specs=[pl.BlockSpec(memory_space=pltpu.SMEM)] + [vmem] * 5 + [anywhere] * 8,
        out_specs=(vmem, vmem),
        scratch_shapes=[
            pltpu.VMEM((length, heads, wide), BF16),
            pltpu.VMEM((length, heads, wide), BF16),
            pltpu.VMEM((length, heads, val), BF16),
            pltpu.VMEM((heads, val, width), BF16),
            pltpu.VMEM((local_rows, width), BF16),
            pltpu.VMEM((heads, length, wide), BF16),
            pltpu.VMEM((ep, heads, length, wide + val), BF16),
            pltpu.VMEM((chips, width, 4 * unit), BF16),
            pltpu.VMEM((chips, subs, CHUNKS, step, 2 * unit // subs), BF16),
            pltpu.VMEM((2 * half, width), BF16),
            pltpu.VMEM((2, ep - 1, cap, width), BF16),
            pltpu.VMEM((2, local_rows, width), BF16),
            pltpu.VMEM((2, RANKS, local_rows), F32),
            pltpu.VMEM((chips, subs, 2 * half, 2 * unit // subs), BF16),
            pltpu.VMEM((CHUNKS, half, step), BF16),
            pltpu.VMEM((CHUNKS, ep, cap, step), BF16),
            pltpu.VMEM((2, heads, length, 1), F32),
            pltpu.VMEM((2, heads, length, 1), F32),
            pltpu.VMEM((2, heads, length, val), F32),
            pltpu.VMEM((heads, length, val), BF16),
            pltpu.VMEM((2, chips, block, width), BF16),
            pltpu.VMEM((chips, block, width), BF16),
            pltpu.VMEM((chips, block, width), BF16),
            pltpu.VMEM((2, chips, block, width), BF16),
            pltpu.VMEM((2, chips, block, width), BF16),
            pltpu.VMEM((ep, cap, local_rows), BF16),
            pltpu.VMEM((local_rows, ep), F32),
            dma((8,)),
            dma((ep + 1,)),
            dma((ep + 1,)),
            dma((2,)),
            dma((2,)),
            dma((2, ep)),
            dma((2, ep)),
            dma((2, chips, PIECES)),
            dma((chips, PIECES)),
            dma((chips, PIECES)),
            dma((chips, PIECES)),
            dma((2, chips, CHUNKS)),
            dma((chips, CHUNKS)),
            dma((chips, CHUNKS)),
            dma((chips, CHUNKS)),
            dma((chips,)),
            dma((chips,)),
            dma,
            dma,
            dma((2, chips)),
            dma((2, chips)),
            dma((CHUNKS, ep)),
            dma((CHUNKS, ep)),
        ],
        compiler_params=pltpu.CompilerParams(
            collective_id=0, has_side_effects=True, vmem_limit_bytes=62 * 1024 * 1024
        ),
    )(
        mixing,
        head_gain[None],
        norm_gain[None],
        expert_ids.T,
        group_gate[None],
        expert_gate.T,
        queries,
        keys,
        values,
        out_weight,
        tokens_b,
        gate,
        up,
        down_weight[0].reshape(CHUNKS, step, unit),
    )


def solution(mesh):
    placed = (
        P("ep", "tp", None),
        P("ep", "tp", None),
        P("ep", "tp", None),
        P("tp"),
        P(),
        P("tp", None, None),
        P(("ep", "tp"), None),
        P(),
        P(("ep", "tp"), None),
        P(("ep", "tp")),
        P(("ep", "tp"), None),
        P("ep", None, "tp"),
        P("ep", None, "tp"),
        P("ep", None, "tp"),
    )
    return jax.shard_map(
        per_device,
        mesh=mesh,
        in_specs=placed,
        out_specs=(P(("ep", "tp"), None), P(("ep", "tp"), None)),
        check_vma=False,
    )
```

```python
import functools
import math

import jax
import jax.numpy as jnp
from jax import lax
from jax.experimental import pallas as pl
from jax.experimental.pallas import tpu as pltpu
from jax.sharding import PartitionSpec as P

HEAD = 64
CHUNKS = 8
PIECES = 2
RANKS = 16
F32 = jnp.float32
BF16 = jnp.bfloat16
MESH = pl.DeviceIdType.MESH
NT = (((1,), (1,)), ((), ()))
TN = (((0,), (0,)), ((), ()))


def kernel(
    ep,
    tp,
    mix_ref,
    gain_ref,
    norm_ref,
    ids_ref,
    group_ref,
    gates_ref,
    q_in,
    k_in,
    v_in,
    ow_in,
    tok_in,
    gate_ref,
    up_ref,
    dn_ref,
    mixed_ref,
    routed_ref,
    q_raw,
    k_raw,
    v_raw,
    ow_ref,
    tok_ref,
    q_ref,
    kv_all,
    w_gu,
    w_dn,
    rows_x,
    out_ref,
    nrm,
    rank_ref,
    hid,
    back,
    ret,
    top_ref,
    sum_ref,
    val_ref,
    att,
    part,
    pair,
    chip_sum,
    landed,
    line_out,
    take_ref,
    local_sem,
    kv_s,
    kv_r,
    t_s,
    t_r,
    x_s,
    x_r,
    gu_s,
    gu_r,
    sg_s,
    sg_r,
    dn_s,
    dn_r,
    sd_s,
    sd_r,
    h_s,
    h_r,
    pr_s,
    pr_r,
    rs_s,
    rs_r,
    b_s,
    b_r,
):
    chips = tp // 2
    me = lax.axis_index("ep")
    mine = lax.axis_index("tp")
    z = mine // 2
    core = mine % 2
    other = z * 2 + 1 - core
    inward = 1 - 2 * (z // (chips // 2))
    heads, length, wide = q_ref.shape
    val = val_ref.shape[3]
    local_rows, width = tok_ref.shape
    half = rows_x.shape[0] // 2
    cap = half // ep
    step = w_dn.shape[3]
    lanes = w_gu.shape[2] // 2
    unit = lanes // 2
    subs = w_dn.shape[1]
    deep = width // PIECES
    joined = gate_ref.shape[1] != unit
    inner = (z >= 1) & (z <= chips - 2)
    is_end = (z == 0) | (z == chips - 1)
    has_guest = (z == 1) | (z == chips - 2)

    def remote(src, dst, send, recv, target):
        return pltpu.make_async_remote_copy(
            src_ref=src,
            dst_ref=dst,
            send_sem=send,
            recv_sem=recv,
            device_id=target,
            device_id_type=MESH,
        )

    if joined:
        own_gu = [pltpu.make_async_copy(gate_ref, w_gu.at[z, :, pl.ds(0, lanes)], local_sem.at[0])]
    else:
        own_gu = [
            pltpu.make_async_copy(gate_ref, w_gu.at[z, :, pl.ds(0, unit)], local_sem.at[0]),
            pltpu.make_async_copy(up_ref, w_gu.at[z, :, pl.ds(unit, unit)], local_sem.at[1]),
        ]
    if subs == 1:
        own_dn = pltpu.make_async_copy(dn_ref, w_dn.at[z, 0, :, :, pl.ds(0, unit)], local_sem.at[2])
    else:
        own_dn = pltpu.make_async_copy(dn_ref, w_dn.at[z, 0], local_sem.at[2])
    own_kv = [
        pltpu.make_async_copy(k_in, k_raw, local_sem.at[3]),
        pltpu.make_async_copy(v_in, v_raw, local_sem.at[4]),
        pltpu.make_async_copy(q_in, q_raw, local_sem.at[5]),
    ]
    own_tok = pltpu.make_async_copy(tok_in, tok_ref, local_sem.at[6])
    own_ow = pltpu.make_async_copy(ow_in, ow_ref, local_sem.at[7])

    barrier = pltpu.get_barrier_semaphore()
    for s in range(1, ep):
        pl.semaphore_signal(
            barrier, inc=1, device_id={"ep": (me + s) % ep}, device_id_type=MESH
        )
    for s in range(1, tp):
        pl.semaphore_signal(
            barrier, inc=1, device_id={"tp": (mine + s) % tp}, device_id_type=MESH
        )
    for copy in [own_tok] + own_gu + own_kv + [own_dn, own_ow]:
        copy.start()
    pl.semaphore_wait(barrier, ep + tp - 2)

    def on_line(at):
        return (at >= 0) & (at <= chips - 1)

    def wants_gu(at):
        return (at >= 1) & (at <= chips - 2)

    def gu_part(src, j):
        return w_gu.at[src, pl.ds(j * deep, deep), pl.ds(0, lanes)]

    def gu_copy(src, j, way):
        return remote(
            gu_part(src, j),
            gu_part(src, j),
            gu_s.at[(1 - way) // 2, src, j],
            gu_r.at[src, j],
            {"tp": (z + way) * 2 + core},
        )

    def sg_copy(src, j):
        return remote(
            gu_part(src, j),
            w_gu.at[src, pl.ds(j * deep, deep), pl.ds(lanes, lanes)],
            sg_s.at[src, j],
            sg_r.at[src, j],
            {"tp": other},
        )

    def dn_part(src, c, which):
        if subs == 1:
            return w_dn.at[src, 0, c, :, pl.ds(which * unit, unit)]
        return w_dn.at[src, which, c]

    def dn_copy(src, c, way):
        return remote(
            dn_part(src, c, 0),
            dn_part(src, c, 0),
            dn_s.at[(1 - way) // 2, src, c],
            dn_r.at[src, c],
            {"tp": (z + way) * 2 + core},
        )

    def sd_copy(src, c):
        return remote(
            dn_part(src, c, 0), dn_part(src, c, 1), sd_s.at[src, c], sd_r.at[src, c], {"tp": other}
        )

    def start_own():
        for copy in own_gu:
            copy.wait()
        for way in (inward, -inward):

            @pl.when(wants_gu(z + way))
            def _(way=way):
                for j in range(PIECES):
                    gu_copy(z, j, way).start()

        @pl.when(inner)
        def _():
            for j in range(PIECES):
                sg_copy(z, j).start()

        own_dn.wait()

        @pl.when(is_end)
        def _():
            for c in range(CHUNKS):
                dn_copy(z, c, inward).start()

        @pl.when(inner)
        def _():
            for c in range(CHUNKS):
                dn_copy(z, c, -inward).start()

        for c in range(CHUNKS):
            sd_copy(z, c).start()

    def source(k, near):
        return (z + k * inward, -inward) if near else (z - k * inward, inward)

    def pass_gu(k, near, j):
        src, way = source(k, near)

        @pl.when(inner & on_line(src))
        def _():
            gu_copy(src, j, way).wait_recv()
            pl.when(wants_gu(z + way))(lambda: gu_copy(src, j, way).start())
            sg_copy(src, j).start()

    def ready_gu(src):
        for j in range(PIECES):
            sg_copy(src, j).wait_recv()

    def pass_dn(k, near, c):
        src, way = source(k, near)

        @pl.when(on_line(src))
        def _():
            dn_copy(src, c, way).wait_recv()
            pl.when(on_line(z + way))(lambda: dn_copy(src, c, way).start())
            sd_copy(src, c).start()

    square_plane = ep == 4
    mid_rows = length // 2

    def kv_move(src, dst, sem, target):
        return remote(src, dst, kv_s.at[sem], kv_r.at[sem], {"ep": target})

    def kv_copy(s):
        return kv_move(kv_all.at[0], kv_all.at[s], s, lax.rem(me + s, ep))

    def kv_half(s, i):
        rows = pl.ds(i * mid_rows, mid_rows)
        return kv_move(kv_all.at[s, :, rows], kv_all.at[3, :, rows], 3 + i, 3)

    def kv_corner(s, i):
        rows = pl.ds(i * mid_rows, mid_rows)
        return kv_move(kv_all.at[s, :, rows], kv_all.at[1, :, rows], 3 + i, 2)

    def kv_lent():
        rows = pl.ds(mid_rows, mid_rows)
        return kv_move(kv_all.at[0, :, rows], kv_all.at[1, :, rows], 1, 0)

    if square_plane:
        near_sends = [((me == 0) | (me == 2), 1), (me <= 1, 2)]
        far_sends = [
            (me == 1, lambda: kv_half(1, 0)),
            (me == 2, lambda: kv_half(2, 1)),
            (me == 3, lambda: kv_corner(2, 0)),
            (me == 0, lambda: kv_corner(1, 1)),
        ]
        early_blocks = [((me == 1) | (me == 3), 1), (me >= 2, 2)]
        late_blocks = [(me >= 2, jnp.where(me == 2, 1, 3))]
    else:
        near_sends = [(me + s < ep, s) for s in range(1, ep - 1)]
        far_sends = [(me + ep - 1 < ep, lambda: kv_copy(ep - 1))]
        early_blocks = [(me >= s, s) for s in range(1, ep - 1)]
        late_blocks = [(me >= ep - 1, ep - 1)]

    def send_near():
        for sends, s in near_sends:
            pl.when(sends)(lambda s=s: kv_copy(s).start())
        if square_plane:
            pl.when(me == 1)(lambda: kv_lent().start())

    def receive_near():
        for has, s in early_blocks:
            pl.when(has)(lambda s=s: kv_copy(s).wait_recv())
        if square_plane:
            pl.when(me == 0)(lambda: kv_lent().wait_recv())

    def send_far():
        for sends, copy in far_sends:
            pl.when(sends)(lambda copy=copy: copy().start())

    def receive_far():
        if square_plane:

            @pl.when(me == 2)
            def _():
                kv_corner(2, 0).wait_recv()
                kv_corner(1, 1).wait_recv()

            @pl.when(me == 3)
            def _():
                kv_half(1, 0).wait_recv()
                kv_half(2, 1).wait_recv()

        else:
            pl.when(me >= ep - 1)(lambda: kv_copy(ep - 1).wait_recv())

    pl.when(inner)(start_own)
    own_tok.wait()

    relative = ids_ref[...] - me
    relative = jnp.where(relative < 0, relative + ep, relative)
    table = (RANKS, local_rows)
    expert_row = lax.broadcasted_iota(jnp.int32, table, 0)
    named = jnp.zeros(table, F32)
    route = jnp.zeros(table, F32)
    for k in range(ids_ref.shape[0]):
        hit = expert_row == relative[k : k + 1, :]
        named = jnp.where(hit, 1.0, named)
        route = route + jnp.where(hit, group_ref[...] * gates_ref[k : k + 1, :], 0.0)
    square = (local_rows, local_rows)
    row_at = lax.broadcasted_iota(jnp.int32, square, 0)
    col_at = lax.broadcasted_iota(jnp.int32, square, 1)
    before = jnp.where(row_at < col_at, 1.0, 0.0).astype(BF16)
    rank = jnp.dot(named.astype(BF16), before, preferred_element_type=F32)
    rank_ref[0] = jnp.where(named > 0.5, rank, -1.0)
    tokens = tok_ref[...].astype(F32)
    nrm[0] = (
        tokens
        * lax.rsqrt(jnp.mean(tokens * tokens, axis=1, keepdims=True) + 1e-06)
        * norm_ref[...]
    ).astype(BF16)

    def guest_copies():
        target = {"tp": (z + inward) * 2 + core}
        return (
            remote(nrm.at[0], nrm.at[1], t_s.at[0], t_r.at[0], target),
            remote(rank_ref.at[0], rank_ref.at[1], t_s.at[1], t_r.at[1], target),
        )

    @pl.when(is_end)
    def _():
        for copy in guest_copies():
            copy.start()
        start_own()

    for copy in own_kv:
        copy.wait()
    part_rows = min(128, length)

    def lay_kv(t, carry):
        rows = pl.ds(pl.multiple_of(t * part_rows, part_rows), part_rows)
        k_flat = k_raw[rows].reshape(part_rows, heads * wide)
        v_flat = v_raw[rows].reshape(part_rows, heads * val)
        for h in range(heads):
            kv_all[0, h, rows, :wide] = k_flat[:, h * wide : (h + 1) * wide]
            kv_all[0, h, rows, wide:] = v_flat[:, h * val : (h + 1) * val]
        return carry

    def lay_q(t, carry):
        rows = pl.ds(pl.multiple_of(t * part_rows, part_rows), part_rows)
        q_flat = q_raw[rows].reshape(part_rows, heads * wide)
        for h in range(heads):
            q = q_flat[:, h * wide : (h + 1) * wide].astype(F32) * (1.0 / math.sqrt(HEAD))
            q_ref[h, rows, :] = q.astype(BF16)
        return carry

    lax.fori_loop(0, length // part_rows, lay_kv, 0)
    send_near()
    lax.fori_loop(0, length // part_rows, lay_q, 0)

    def x_copy(g, s):
        return remote(
            out_ref.at[g, s - 1],
            rows_x.at[pl.ds(g * half + s * cap, cap)],
            x_s.at[g, s],
            x_r.at[g, s],
            {"ep": lax.rem(me + s, ep)},
        )

    slot_row = lax.broadcasted_iota(jnp.int32, (cap, local_rows), 0).astype(F32)

    def place_of(g, s):
        return jnp.where(rank_ref[g, s : s + 1, :] == slot_row, 1.0, 0.0).astype(BF16)

    def dispatch(g):
        for s in list(range(1, ep)) + [0]:
            place = place_of(g, s)
            for n in range(CHUNKS):
                cols = slice(n * step, (n + 1) * step)
                picked = jnp.dot(place, nrm[g, :, cols], preferred_element_type=F32).astype(BF16)
                if s:
                    out_ref[g, s - 1, :, cols] = picked
                else:
                    rows_x[g * half : g * half + cap, cols] = picked
            if s:
                x_copy(g, s).start()

    tile = min(256, length)
    tiles = length // tile

    def attend(s, first=False):
        block = kv_all.at[s]

        def one(index, carry):
            h = index // tiles
            start = pl.multiple_of((index % tiles) * tile, tile)
            rows = pl.ds(start, tile)
            q = q_ref[h, rows, :]
            lane = lax.broadcasted_iota(jnp.int32, (tile, wide), 1)
            for m in range(2):
                pick = (lane < HEAD) if m == 0 else (lane >= HEAD)
                q_map = jnp.where(pick, q, jnp.zeros_like(q))
                scores = lax.dot_general(q_map, block[h, :, :wide], NT, preferred_element_type=F32)
                if first:
                    row = start + lax.broadcasted_iota(jnp.int32, scores.shape, 0)
                    col = lax.broadcasted_iota(jnp.int32, scores.shape, 1)
                    scores = jnp.where(col <= row, scores, -1e30)
                    fresh = jnp.max(scores, axis=1, keepdims=True)
                else:
                    top = top_ref[m, h, rows, :]
                    fresh = jnp.maximum(top, jnp.max(scores, axis=1, keepdims=True))
                expo = jnp.exp(scores - fresh)
                total = jnp.sum(expo, axis=1, keepdims=True)
                value = jnp.dot(
                    expo.astype(BF16), block[h, :, wide:], preferred_element_type=F32
                )
                if not first:
                    shrink = jnp.exp(top - fresh)
                    total = total + sum_ref[m, h, rows, :] * shrink
                    value = value + val_ref[m, h, rows, :] * shrink
                top_ref[m, h, rows, :] = fresh
                sum_ref[m, h, rows, :] = total
                val_ref[m, h, rows, :] = value
            return carry

        lax.fori_loop(0, heads * tiles, one, 0)

    attend(0, True)

    slot_at = lax.broadcasted_iota(jnp.int32, (local_rows, half), 1).astype(F32)
    weight = jnp.zeros((local_rows, half), F32)
    diagonal = row_at == col_at
    for s in range(ep):
        rank_col = jnp.sum(jnp.where(diagonal, rank_ref[0, s : s + 1, :], 0.0), axis=1, keepdims=True)
        route_col = jnp.sum(jnp.where(diagonal, route[s : s + 1, :], 0.0), axis=1, keepdims=True)
        lane_of = jnp.where(rank_col >= 0.0, rank_col + float(s * cap), -1.0)
        weight = jnp.where(slot_at == lane_of, route_col, weight)
    upper = weight.astype(BF16)
    take_ref[0] = upper
    take_ref[1] = (weight - upper.astype(F32)).astype(BF16)

    m_tile = half // 2

    def hidden_of(src, first, count):
        def one(t, carry):
            rows = pl.ds(pl.multiple_of(t * m_tile, m_tile), m_tile)
            product = jnp.dot(rows_x[rows, :], w_gu[src], preferred_element_type=F32)
            for i in range(2):
                gate = product[:, i * lanes : i * lanes + unit]
                value = gate / (1.0 + jnp.exp(-gate)) * product[:, i * lanes + unit : (i + 1) * lanes]
                if subs == 1:
                    hid[src, 0, rows, i * unit : (i + 1) * unit] = value.astype(BF16)
                else:
                    hid[src, i, rows, :] = value.astype(BF16)
            return carry

        lax.fori_loop(first, first + count, one, 0)

    def h_copy(src):
        return remote(
            hid.at[src, :, pl.ds(half, half)],
            hid.at[src, :, pl.ds(0, half)],
            h_s.at[src],
            h_r.at[src],
            {"tp": (z - inward) * 2 + core},
        )

    def finish(index, carry):
        h = index // tiles
        rows = pl.ds(pl.multiple_of((index % tiles) * tile, tile), tile)
        diff = val_ref[0, h, rows, :] / sum_ref[0, h, rows, :] - mix_ref[h] * (
            val_ref[1, h, rows, :] / sum_ref[1, h, rows, :]
        )
        scaled = diff * lax.rsqrt(jnp.mean(diff * diff, axis=1, keepdims=True) + 1e-05)
        att[h, rows, :] = (scaled * gain_ref[...]).astype(BF16)
        return carry

    block = length // tp

    def project(t, carry):
        rows = pl.ds(pl.multiple_of(t * 2 * block, 2 * block), 2 * block)
        total = 0.0
        for h in range(heads):
            total = total + jnp.dot(att[h, rows, :], ow_ref[h], preferred_element_type=F32)
        part[0, t] = total[:block].astype(BF16)
        part[1, t] = total[block:].astype(BF16)
        return carry

    pair_copy = remote(part.at[1 - core], pair, pr_s, pr_r, {"tp": other})

    def add_pair(t, carry):
        chip_sum[t] = (part[core, t].astype(F32) + pair[t].astype(F32)).astype(BF16)
        return carry

    def line_copy(side, t, first):
        return remote(
            chip_sum.at[t] if first else line_out.at[side, t],
            landed.at[side, t],
            rs_s.at[side, t],
            rs_r.at[side, t],
            {"tp": (z + 1 - 2 * side) * 2 + core},
        )

    def stage_each(k, do):
        for side in range(2):
            at = k if side == 0 else chips - 1 - k
            targets = range(chips - 1, k, -1) if side == 0 else range(chips - 1 - k)

            @pl.when(z == at)
            def _(side=side, targets=targets):
                for t in targets:
                    do(side, t, k == 0)

    def stage_send(side, t, first):
        copy = line_copy(side, t, first)
        if not first:
            copy.wait_recv()
            line_out[side, t] = (
                chip_sum[t].astype(F32) + landed[side, t].astype(F32)
            ).astype(BF16)
        copy.start()

    def back_copy(c, s):
        return remote(
            back.at[c, pl.ds(s * cap, cap)],
            ret.at[c, pl.ds(s * cap, cap)],
            b_s.at[c, s],
            b_r.at[c, s],
            {"ep": lax.rem(me + ep - s, ep)},
        )

    def down_of(c):
        total = 0.0
        for src in range(chips):
            for i in range(subs):
                total = total + lax.dot_general(
                    hid[src, i, :half, :], w_dn[src, i, c], NT, preferred_element_type=F32
                )
        result = total.astype(BF16)
        ret[c, :cap, :] = result[:cap]
        back[c, cap:, :] = result[cap:]

    def combine(c):
        for s in range(1, ep):
            back_copy(c, s).wait_recv()
        total = jnp.dot(take_ref[0], ret[c], preferred_element_type=F32)
        total = total + jnp.dot(take_ref[1], ret[c], preferred_element_type=F32)
        routed_ref[:, c * step : (c + 1) * step] = total.astype(BF16)

    def give_back(c):
        for src in range(chips):
            sd_copy(src, c).wait_recv()
        down_of(c)
        for s in range(1, ep):
            back_copy(c, s).start()

    def own_hidden(first, last):
        lax.fori_loop(first, last, lambda src, carry: (hidden_of(src, 0, 2), carry)[1], 0)

    def guest_hidden(src):
        hidden_of(src, 2, 2)
        h_copy(src).start()

    def pass_rest(c):
        for k in range(1, chips):
            for near in (True, False):
                if k > 1 or near:
                    pass_dn(k, near, c)

    def start_mixed():
        lax.fori_loop(0, heads * tiles, finish, 0)
        own_ow.wait()
        lax.fori_loop(0, chips, project, 0)
        pair_copy.start()

    def chip_mixed():
        pair_copy.wait_recv()
        lax.fori_loop(0, chips, add_pair, 0)

    def attend_far():
        receive_far()
        for has, s in late_blocks:
            pl.when(has)(lambda s=s: attend(s))

    @pl.when(has_guest)
    def _():
        for copy in guest_copies():
            copy.wait_recv()
        dispatch(1)

    receive_near()
    send_far()
    for has, s in early_blocks:
        pl.when(has)(lambda s=s: attend(s))

    @pl.when(inner)
    def _():
        for j in range(PIECES):
            pass_gu(1, True, j)
        for j in range(PIECES - 1):
            pass_gu(1, False, j)
        ready_gu(z)
        ready_gu(z + inward)

    @pl.when(has_guest)
    def _():
        for s in range(1, ep):
            x_copy(1, s).wait_recv()
        guest_hidden(z)
        guest_hidden(z + inward)

    @pl.when(inner)
    def _():
        dispatch(0)
        pass_gu(1, False, PIECES - 1)
        ready_gu(z - inward)
        pl.when(has_guest)(lambda: guest_hidden(z - inward))
        for c in range(CHUNKS):
            if c == CHUNKS // 2:
                attend_far()
            dn_copy(z, c, inward).start()
            pass_dn(1, False, c)
        for k in range(2, chips):
            for near in (True, False):
                for j in range(PIECES):
                    pass_gu(k, near, j)
                far = source(k, near)[0]

                @pl.when(on_line(far))
                def _(far=far):
                    ready_gu(far)
                    pl.when(has_guest)(lambda: guest_hidden(far))

        pass_rest(0)
        start_mixed()
        pass_rest(1)
        for s in range(1, ep):
            x_copy(0, s).wait_recv()
        own_hidden(0, chips // 2)
        pass_rest(2)
        own_hidden(chips // 2, chips)
        pass_rest(3)
        chip_mixed()
        for c in range(4):
            give_back(c)
        stage_each(1, stage_send)
        for c in range(4, CHUNKS):
            pass_rest(c)
            give_back(c)

    @pl.when(is_end)
    def _():
        attend_far()
        start_mixed()
        chip_mixed()
        stage_each(0, stage_send)
        pass_rest(0)
        for src in range(chips):
            h_copy(src).wait_recv()
        give_back(0)
        for c in range(1, CHUNKS):
            pass_rest(c)
            give_back(c)

    for c in range(CHUNKS):
        if c == CHUNKS // 2:
            for k in range(2, chips - 1):
                stage_each(k, stage_send)
        combine(c)

    mixed_ref[...] = chip_sum[z]
    for side in range(2):

        @pl.when((z > 0) if side == 0 else (z < chips - 1))
        def _(side=side):
            line_copy(side, z, False).wait_recv()
            mixed_ref[...] = (
                mixed_ref[...].astype(F32) + landed[side, z].astype(F32)
            ).astype(BF16)

    for sends, s in near_sends:
        pl.when(sends)(lambda s=s: kv_copy(s).wait_send())
    if square_plane:
        pl.when(me == 1)(lambda: kv_lent().wait_send())
    for sends, copy in far_sends:
        pl.when(sends)(lambda copy=copy: copy().wait_send())
    for s in range(1, ep):

        @pl.when(inner)
        def _(s=s):
            x_copy(0, s).wait_send()

        @pl.when(has_guest)
        def _(s=s):
            x_copy(1, s).wait_send()

    @pl.when(is_end)
    def _():
        for copy in guest_copies():
            copy.wait_send()

    @pl.when(has_guest)
    def _():
        for src in range(chips):
            h_copy(src).wait_send()

    for k in range(chips):
        for near in (True, False):
            src, way = source(k, near)

            @pl.when(on_line(src))
            def _(k=k, near=near, src=src, way=way):
                @pl.when(wants_gu(z + way) & (inner | (k == 0)))
                def _():
                    for j in range(PIECES):
                        gu_copy(src, j, way).wait_send()

                @pl.when(on_line(z + way))
                def _():
                    for c in range(CHUNKS):
                        dn_copy(src, c, way).wait_send()

                if k or near:

                    @pl.when(inner)
                    def _():
                        for j in range(PIECES):
                            sg_copy(src, j).wait_send()

                    for c in range(CHUNKS):
                        sd_copy(src, c).wait_send()

    pair_copy.wait_send()
    for k in range(chips - 1):
        stage_each(k, lambda side, t, first: line_copy(side, t, first).wait_send())
    for c in range(CHUNKS):
        for s in range(1, ep):
            back_copy(c, s).wait_send()


def per_device(
    queries,
    keys,
    values,
    mixing,
    head_gain,
    out_weight,
    tokens_b,
    norm_gain,
    expert_ids,
    group_gate,
    expert_gate,
    gate_weight,
    up_weight,
    down_weight,
):
    ep = lax.axis_size("ep")
    tp = lax.axis_size("tp")
    chips = tp // 2
    length, heads, wide = queries.shape
    val = values.shape[2]
    local_rows, width = tokens_b.shape
    top_count = expert_ids.shape[1]
    unit = gate_weight.shape[2]
    assert gate_weight.shape[0] == 1 and wide == 2 * HEAD and chips >= 4 and ep <= RANKS
    capacity = 3 * local_rows * top_count // (2 * ep)
    cap = -(-capacity // 16) * 16
    step = width // CHUNKS

    gate, up = gate_weight[0], up_weight[0]
    subs = 1
    if unit % 128:
        gate = jnp.concatenate([gate, up], axis=1)
        subs = 2
    half = ep * cap
    block = length // tp
    vmem = pl.BlockSpec(memory_space=pltpu.VMEM)
    anywhere = pl.BlockSpec(memory_space=pl.ANY)
    dma = pltpu.SemaphoreType.DMA
    return pl.pallas_call(
        functools.partial(kernel, ep, tp),
        out_shape=(
            pltpu.VMEM((block, width), BF16),
            pltpu.VMEM((local_rows, width), BF16),
        ),
        in_specs=[pl.BlockSpec(memory_space=pltpu.SMEM)] + [vmem] * 5 + [anywhere] * 8,
        out_specs=(vmem, vmem),
        scratch_shapes=[
            pltpu.VMEM((length, heads, wide), BF16),
            pltpu.VMEM((length, heads, wide), BF16),
            pltpu.VMEM((length, heads, val), BF16),
            pltpu.VMEM((heads, val, width), BF16),
            pltpu.VMEM((local_rows, width), BF16),
            pltpu.VMEM((heads, length, wide), BF16),
            pltpu.VMEM((ep, heads, length, wide + val), BF16),
            pltpu.VMEM((chips, width, 4 * unit), BF16),
            pltpu.VMEM((chips, subs, CHUNKS, step, 2 * unit // subs), BF16),
            pltpu.VMEM((2 * half, width), BF16),
            pltpu.VMEM((2, ep - 1, cap, width), BF16),
            pltpu.VMEM((2, local_rows, width), BF16),
            pltpu.VMEM((2, RANKS, local_rows), F32),
            pltpu.VMEM((chips, subs, 2 * half, 2 * unit // subs), BF16),
            pltpu.VMEM((CHUNKS, half, step), BF16),
            pltpu.VMEM((CHUNKS, half, step), BF16),
            pltpu.VMEM((2, heads, length, 1), F32),
            pltpu.VMEM((2, heads, length, 1), F32),
            pltpu.VMEM((2, heads, length, val), F32),
            pltpu.VMEM((heads, length, val), BF16),
            pltpu.VMEM((2, chips, block, width), BF16),
            pltpu.VMEM((chips, block, width), BF16),
            pltpu.VMEM((chips, block, width), BF16),
            pltpu.VMEM((2, chips, block, width), BF16),
            pltpu.VMEM((2, chips, block, width), BF16),
            pltpu.VMEM((2, local_rows, half), BF16),
            dma((8,)),
            dma((ep + 1,)),
            dma((ep + 1,)),
            dma((2,)),
            dma((2,)),
            dma((2, ep)),
            dma((2, ep)),
            dma((2, chips, PIECES)),
            dma((chips, PIECES)),
            dma((chips, PIECES)),
            dma((chips, PIECES)),
            dma((2, chips, CHUNKS)),
            dma((chips, CHUNKS)),
            dma((chips, CHUNKS)),
            dma((chips, CHUNKS)),
            dma((chips,)),
            dma((chips,)),
            dma,
            dma,
            dma((2, chips)),
            dma((2, chips)),
            dma((CHUNKS, ep)),
            dma((CHUNKS, ep)),
        ],
        compiler_params=pltpu.CompilerParams(
            collective_id=0, has_side_effects=True, vmem_limit_bytes=62 * 1024 * 1024
        ),
    )(
        mixing,
        head_gain[None],
        norm_gain[None],
        expert_ids.T,
        group_gate[None],
        expert_gate.T,
        queries,
        keys,
        values,
        out_weight,
        tokens_b,
        gate,
        up,
        down_weight[0].reshape(CHUNKS, step, unit),
    )


def solution(mesh):
    placed = (
        P("ep", "tp", None),
        P("ep", "tp", None),
        P("ep", "tp", None),
        P("tp"),
        P(),
        P("tp", None, None),
        P(("ep", "tp"), None),
        P(),
        P(("ep", "tp"), None),
        P(("ep", "tp")),
        P(("ep", "tp"), None),
        P("ep", None, "tp"),
        P("ep", None, "tp"),
        P("ep", None, "tp"),
    )
    return jax.shard_map(
        per_device,
        mesh=mesh,
        in_specs=placed,
        out_specs=(P(("ep", "tp"), None), P(("ep", "tp"), None)),
        check_vma=False,
    )
```

```python
import functools
import math

import jax
import jax.numpy as jnp
from jax import lax
from jax.experimental import pallas as pl
from jax.experimental.pallas import tpu as pltpu
from jax.sharding import PartitionSpec as P

HEAD = 64
CHUNKS = 8
LATE = 6
PIECES = 2
RANKS = 16
F32 = jnp.float32
BF16 = jnp.bfloat16
MESH = pl.DeviceIdType.MESH
NT = (((1,), (1,)), ((), ()))
TN = (((0,), (0,)), ((), ()))


def kernel(
    ep,
    tp,
    mix_ref,
    gain_ref,
    norm_ref,
    ids_ref,
    group_ref,
    gates_ref,
    q_in,
    k_in,
    v_in,
    ow_in,
    tok_in,
    gate_ref,
    up_ref,
    dn_ref,
    mixed_ref,
    routed_ref,
    q_raw,
    k_raw,
    v_raw,
    ow_ref,
    tok_ref,
    q_ref,
    kv_all,
    w_gu,
    w_dn,
    rows_x,
    out_ref,
    nrm,
    rank_ref,
    hid,
    back,
    ret,
    top_ref,
    sum_ref,
    val_ref,
    att,
    part,
    pair,
    chip_sum,
    landed,
    line_out,
    take_ref,
    local_sem,
    kv_s,
    kv_r,
    t_s,
    t_r,
    x_s,
    x_r,
    gu_s,
    gu_r,
    sg_s,
    sg_r,
    dn_s,
    dn_r,
    sd_s,
    sd_r,
    h_s,
    h_r,
    pr_s,
    pr_r,
    rs_s,
    rs_r,
    b_s,
    b_r,
):
    chips = tp // 2
    me = lax.axis_index("ep")
    mine = lax.axis_index("tp")
    z = mine // 2
    core = mine % 2
    other = z * 2 + 1 - core
    inward = 1 - 2 * (z // (chips // 2))
    heads, length, wide = q_ref.shape
    val = val_ref.shape[3]
    local_rows, width = tok_ref.shape
    half = rows_x.shape[0] // 2
    cap = half // ep
    step = w_dn.shape[3]
    lanes = w_gu.shape[2] // 2
    unit = lanes // 2
    subs = w_dn.shape[1]
    deep = width // PIECES
    joined = gate_ref.shape[1] != unit
    inner = (z >= 1) & (z <= chips - 2)
    is_end = (z == 0) | (z == chips - 1)
    has_guest = (z == 1) | (z == chips - 2)

    def remote(src, dst, send, recv, target):
        return pltpu.make_async_remote_copy(
            src_ref=src,
            dst_ref=dst,
            send_sem=send,
            recv_sem=recv,
            device_id=target,
            device_id_type=MESH,
        )

    if joined:
        own_gu = [pltpu.make_async_copy(gate_ref, w_gu.at[z, :, pl.ds(0, lanes)], local_sem.at[0])]
    else:
        own_gu = [
            pltpu.make_async_copy(gate_ref, w_gu.at[z, :, pl.ds(0, unit)], local_sem.at[0]),
            pltpu.make_async_copy(up_ref, w_gu.at[z, :, pl.ds(unit, unit)], local_sem.at[1]),
        ]
    if subs == 1:
        own_dn = pltpu.make_async_copy(dn_ref, w_dn.at[z, 0, :, :, pl.ds(0, unit)], local_sem.at[2])
    else:
        own_dn = pltpu.make_async_copy(dn_ref, w_dn.at[z, 0], local_sem.at[2])
    own_kv = [
        pltpu.make_async_copy(k_in, k_raw, local_sem.at[3]),
        pltpu.make_async_copy(v_in, v_raw, local_sem.at[4]),
        pltpu.make_async_copy(q_in, q_raw, local_sem.at[5]),
    ]
    own_tok = pltpu.make_async_copy(tok_in, tok_ref, local_sem.at[6])
    own_ow = pltpu.make_async_copy(ow_in, ow_ref, local_sem.at[7])

    barrier = pltpu.get_barrier_semaphore()
    for s in range(1, ep):
        pl.semaphore_signal(
            barrier, inc=1, device_id={"ep": (me + s) % ep}, device_id_type=MESH
        )
    pl.semaphore_signal(barrier, inc=1, device_id={"tp": other}, device_id_type=MESH)
    for way in (-1, 1):

        @pl.when((z + way >= 0) & (z + way <= chips - 1))
        def _(way=way):
            pl.semaphore_signal(
                barrier,
                inc=1,
                device_id={"tp": (z + way) * 2 + core},
                device_id_type=MESH,
            )

    for copy in [own_tok] + own_gu + own_kv + [own_dn, own_ow]:
        copy.start()
    on_sides = (z + chips - 1) // chips + (2 * chips - 2 - z) // chips
    pl.semaphore_wait(barrier, ep + on_sides)

    def on_line(at):
        return (at >= 0) & (at <= chips - 1)

    def wants_gu(at):
        return (at >= 1) & (at <= chips - 2)

    def gu_part(src, j):
        return w_gu.at[src, pl.ds(j * deep, deep), pl.ds(0, lanes)]

    def gu_copy(src, j, way):
        return remote(
            gu_part(src, j),
            gu_part(src, j),
            gu_s.at[(1 - way) // 2, src],
            gu_r.at[src, j],
            {"tp": (z + way) * 2 + core},
        )

    def sg_copy(src, j):
        return remote(
            gu_part(src, j),
            w_gu.at[src, pl.ds(j * deep, deep), pl.ds(lanes, lanes)],
            sg_s.at[src],
            sg_r.at[src, j],
            {"tp": other},
        )

    def dn_part(src, c, which):
        if subs == 1:
            return w_dn.at[src, 0, c, :, pl.ds(which * unit, unit)]
        return w_dn.at[src, which, c]

    def dn_copy(src, c, way):
        return remote(
            dn_part(src, c, 0),
            dn_part(src, c, 0),
            dn_s.at[(1 - way) // 2, src],
            dn_r.at[src, c],
            {"tp": (z + way) * 2 + core},
        )

    def sd_copy(src, c):
        return remote(
            dn_part(src, c, 0), dn_part(src, c, 1), sd_s.at[src], sd_r.at[c], {"tp": other}
        )

    def gu_sent(src, way):
        whole = w_gu.at[src, :, pl.ds(0, lanes)]
        sem = gu_s.at[(1 - way) // 2, src]
        remote(whole, whole, sem, gu_r.at[src, 0], {"tp": other}).wait_send()

    def sg_sent(src):
        whole = w_gu.at[src, :, pl.ds(0, lanes)]
        remote(whole, whole, sg_s.at[src], sg_r.at[src, 0], {"tp": other}).wait_send()

    def dn_whole(src):
        if subs == 1:
            return w_dn.at[src, 0, :, :, pl.ds(0, unit)]
        return w_dn.at[src, 0]

    def dn_sent(src, way):
        whole, sem = dn_whole(src), dn_s.at[(1 - way) // 2, src]
        remote(whole, whole, sem, dn_r.at[src, 0], {"tp": other}).wait_send()

    def sd_sent(src):
        whole = dn_whole(src)
        remote(whole, whole, sd_s.at[src], sd_r.at[0], {"tp": other}).wait_send()

    def start_own():
        for copy in own_gu:
            copy.wait()
        for way in (inward, -inward):

            @pl.when(wants_gu(z + way))
            def _(way=way):
                for j in range(PIECES):
                    gu_copy(z, j, way).start()

        @pl.when(inner)
        def _():
            for j in range(PIECES):
                sg_copy(z, j).start()

        own_dn.wait()

        @pl.when(is_end)
        def _():
            for c in range(CHUNKS):
                dn_copy(z, c, inward).start()

        @pl.when(inner)
        def _():
            for c in range(CHUNKS):
                dn_copy(z, c, -inward).start()
            for c in range(LATE, CHUNKS):
                dn_copy(z, c, inward).start()

        for c in range(CHUNKS):
            sd_copy(z, c).start()

    def source(k, near):
        return (z + k * inward, -inward) if near else (z - k * inward, inward)

    def pass_gu(k, near, j):
        src, way = source(k, near)

        @pl.when(inner & on_line(src))
        def _():
            gu_copy(src, j, way).wait_recv()
            pl.when(wants_gu(z + way))(lambda: gu_copy(src, j, way).start())
            sg_copy(src, j).start()

    def ready_gu(src):
        for j in range(PIECES):
            sg_copy(src, j).wait_recv()

    def pass_dn(k, near, c):
        src, way = source(k, near)

        @pl.when(on_line(src))
        def _():
            dn_copy(src, c, way).wait_recv()
            pl.when(on_line(z + way))(lambda: dn_copy(src, c, way).start())
            sd_copy(src, c).start()

    square_plane = ep == 4
    mid_rows = length // 2

    def kv_move(src, dst, sem, target):
        return remote(src, dst, kv_s.at[sem], kv_r.at[sem], {"ep": target})

    def kv_copy(s):
        return kv_move(kv_all.at[0], kv_all.at[s], s, lax.rem(me + s, ep))

    def kv_half(s, i):
        rows = pl.ds(i * mid_rows, mid_rows)
        return kv_move(kv_all.at[s, :, rows], kv_all.at[3, :, rows], 3 + i, 3)

    def kv_corner(s, i):
        rows = pl.ds(i * mid_rows, mid_rows)
        return kv_move(kv_all.at[s, :, rows], kv_all.at[1, :, rows], 3 + i, 2)

    def kv_lent():
        rows = pl.ds(mid_rows, mid_rows)
        return kv_move(kv_all.at[0, :, rows], kv_all.at[1, :, rows], 1, 0)

    if square_plane:
        near_sends = [((me == 0) | (me == 2), 1), (me <= 1, 2)]
        far_sends = [
            (me == 1, lambda: kv_half(1, 0)),
            (me == 2, lambda: kv_half(2, 1)),
            (me == 3, lambda: kv_corner(2, 0)),
            (me == 0, lambda: kv_corner(1, 1)),
        ]
        early_blocks = [((me == 1) | (me == 3), 1), (me >= 2, 2)]
        late_blocks = [(me >= 2, jnp.where(me == 2, 1, 3))]
    else:
        near_sends = [(me + s < ep, s) for s in range(1, ep - 1)]
        far_sends = [(me + ep - 1 < ep, lambda: kv_copy(ep - 1))]
        early_blocks = [(me >= s, s) for s in range(1, ep - 1)]
        late_blocks = [(me >= ep - 1, ep - 1)]

    def send_near():
        for sends, s in near_sends:
            pl.when(sends)(lambda s=s: kv_copy(s).start())
        if square_plane:
            pl.when(me == 1)(lambda: kv_lent().start())

    def receive_near():
        for has, s in early_blocks:
            pl.when(has)(lambda s=s: kv_copy(s).wait_recv())
        if square_plane:
            pl.when(me == 0)(lambda: kv_lent().wait_recv())

    def send_far():
        for sends, copy in far_sends:
            pl.when(sends)(lambda copy=copy: copy().start())

    def receive_far():
        if square_plane:

            @pl.when(me == 2)
            def _():
                kv_corner(2, 0).wait_recv()
                kv_corner(1, 1).wait_recv()

            @pl.when(me == 3)
            def _():
                kv_half(1, 0).wait_recv()
                kv_half(2, 1).wait_recv()

        else:
            pl.when(me >= ep - 1)(lambda: kv_copy(ep - 1).wait_recv())

    pl.when(inner)(start_own)
    own_tok.wait()

    relative = ids_ref[...] - me
    relative = jnp.where(relative < 0, relative + ep, relative)
    table = (RANKS, local_rows)
    expert_row = lax.broadcasted_iota(jnp.int32, table, 0)
    named = jnp.zeros(table, F32)
    route = jnp.zeros(table, F32)
    for k in range(ids_ref.shape[0]):
        hit = expert_row == relative[k : k + 1, :]
        named = jnp.where(hit, 1.0, named)
        route = route + jnp.where(hit, group_ref[...] * gates_ref[k : k + 1, :], 0.0)
    square = (local_rows, local_rows)
    row_at = lax.broadcasted_iota(jnp.int32, square, 0)
    col_at = lax.broadcasted_iota(jnp.int32, square, 1)
    before = jnp.where(row_at < col_at, 1.0, 0.0).astype(BF16)
    rank = jnp.dot(named.astype(BF16), before, preferred_element_type=F32)
    rank_ref[0] = jnp.where(named > 0.5, rank, -1.0)
    tokens = tok_ref[...].astype(F32)
    nrm[0] = (
        tokens
        * lax.rsqrt(jnp.mean(tokens * tokens, axis=1, keepdims=True) + 1e-06)
        * norm_ref[...]
    ).astype(BF16)

    def guest_copies():
        target = {"tp": (z + inward) * 2 + core}
        return (
            remote(nrm.at[0], nrm.at[1], t_s.at[0], t_r.at[0], target),
            remote(rank_ref.at[0], rank_ref.at[1], t_s.at[1], t_r.at[1], target),
        )

    @pl.when(is_end)
    def _():
        for copy in guest_copies():
            copy.start()
        start_own()

    for copy in own_kv:
        copy.wait()
    part_rows = min(128, length)

    def lay_kv(t, carry):
        rows = pl.ds(pl.multiple_of(t * part_rows, part_rows), part_rows)
        k_flat = k_raw[rows].reshape(part_rows, heads * wide)
        v_flat = v_raw[rows].reshape(part_rows, heads * val)
        for h in range(heads):
            kv_all[0, h, rows, :wide] = k_flat[:, h * wide : (h + 1) * wide]
            kv_all[0, h, rows, wide:] = v_flat[:, h * val : (h + 1) * val]
        return carry

    def lay_q(t, carry):
        rows = pl.ds(pl.multiple_of(t * part_rows, part_rows), part_rows)
        q_flat = q_raw[rows].reshape(part_rows, heads * wide)
        for h in range(heads):
            q = q_flat[:, h * wide : (h + 1) * wide].astype(F32) * (1.0 / math.sqrt(HEAD))
            q_ref[h, rows, :] = q.astype(BF16)
        return carry

    lax.fori_loop(0, length // part_rows, lay_kv, 0)
    send_near()
    lax.fori_loop(0, length // part_rows, lay_q, 0)

    def x_copy(g, s):
        return remote(
            out_ref.at[g, s - 1],
            rows_x.at[pl.ds(g * half + s * cap, cap)],
            x_s.at[g, s],
            x_r.at[g, s],
            {"ep": lax.rem(me + s, ep)},
        )

    slot_row = lax.broadcasted_iota(jnp.int32, (cap, local_rows), 0).astype(F32)

    def place_of(g, s):
        return jnp.where(rank_ref[g, s : s + 1, :] == slot_row, 1.0, 0.0).astype(BF16)

    def dispatch(g):
        for s in list(range(1, ep)) + [0]:
            place = place_of(g, s)
            for n in range(CHUNKS):
                cols = slice(n * step, (n + 1) * step)
                picked = jnp.dot(place, nrm[g, :, cols], preferred_element_type=F32).astype(BF16)
                if s:
                    out_ref[g, s - 1, :, cols] = picked
                else:
                    rows_x[g * half : g * half + cap, cols] = picked
            if s:
                x_copy(g, s).start()

    tile = min(256, length)
    tiles = length // tile

    def attend(s, first=False):
        block = kv_all.at[s]

        def one(index, carry):
            h = index // tiles
            start = pl.multiple_of((index % tiles) * tile, tile)
            rows = pl.ds(start, tile)
            q = q_ref[h, rows, :]
            lane = lax.broadcasted_iota(jnp.int32, (tile, wide), 1)
            for m in range(2):
                pick = (lane < HEAD) if m == 0 else (lane >= HEAD)
                q_map = jnp.where(pick, q, jnp.zeros_like(q))
                scores = lax.dot_general(q_map, block[h, :, :wide], NT, preferred_element_type=F32)
                if first:
                    row = start + lax.broadcasted_iota(jnp.int32, scores.shape, 0)
                    col = lax.broadcasted_iota(jnp.int32, scores.shape, 1)
                    scores = jnp.where(col <= row, scores, -1e30)
                    fresh = jnp.max(scores, axis=1, keepdims=True)
                else:
                    top = top_ref[m, h, rows, :]
                    fresh = jnp.maximum(top, jnp.max(scores, axis=1, keepdims=True))
                expo = jnp.exp(scores - fresh)
                total = jnp.sum(expo, axis=1, keepdims=True)
                value = jnp.dot(
                    expo.astype(BF16), block[h, :, wide:], preferred_element_type=F32
                )
                if not first:
                    shrink = jnp.exp(top - fresh)
                    total = total + sum_ref[m, h, rows, :] * shrink
                    value = value + val_ref[m, h, rows, :] * shrink
                top_ref[m, h, rows, :] = fresh
                sum_ref[m, h, rows, :] = total
                val_ref[m, h, rows, :] = value
            return carry

        lax.fori_loop(0, heads * tiles, one, 0)

    attend(0, True)

    slot_at = lax.broadcasted_iota(jnp.int32, (local_rows, half), 1).astype(F32)
    weight = jnp.zeros((local_rows, half), F32)
    diagonal = row_at == col_at
    for s in range(ep):
        rank_col = jnp.sum(jnp.where(diagonal, rank_ref[0, s : s + 1, :], 0.0), axis=1, keepdims=True)
        route_col = jnp.sum(jnp.where(diagonal, route[s : s + 1, :], 0.0), axis=1, keepdims=True)
        lane_of = jnp.where(rank_col >= 0.0, rank_col + float(s * cap), -1.0)
        weight = jnp.where(slot_at == lane_of, route_col, weight)
    upper = weight.astype(BF16)
    take_ref[0] = upper
    take_ref[1] = (weight - upper.astype(F32)).astype(BF16)

    m_tile = half // 2

    def hidden_of(src, first, count):
        def one(t, carry):
            rows = pl.ds(pl.multiple_of(t * m_tile, m_tile), m_tile)
            product = jnp.dot(rows_x[rows, :], w_gu[src], preferred_element_type=F32)
            for i in range(2):
                gate = product[:, i * lanes : i * lanes + unit]
                value = gate / (1.0 + jnp.exp(-gate)) * product[:, i * lanes + unit : (i + 1) * lanes]
                if subs == 1:
                    hid[src, 0, rows, i * unit : (i + 1) * unit] = value.astype(BF16)
                else:
                    hid[src, i, rows, :] = value.astype(BF16)
            return carry

        lax.fori_loop(first, first + count, one, 0)

    def h_copy(src):
        return remote(
            hid.at[src, :, pl.ds(half, half)],
            hid.at[src, :, pl.ds(0, half)],
            h_s.at[src],
            h_r.at[src],
            {"tp": (z - inward) * 2 + core},
        )

    def finish(index, carry):
        h = index // tiles
        rows = pl.ds(pl.multiple_of((index % tiles) * tile, tile), tile)
        diff = val_ref[0, h, rows, :] / sum_ref[0, h, rows, :] - mix_ref[h] * (
            val_ref[1, h, rows, :] / sum_ref[1, h, rows, :]
        )
        scaled = diff * lax.rsqrt(jnp.mean(diff * diff, axis=1, keepdims=True) + 1e-05)
        att[h, rows, :] = (scaled * gain_ref[...]).astype(BF16)
        return carry

    block = length // tp

    def project(t, carry):
        rows = pl.ds(pl.multiple_of(t * 2 * block, 2 * block), 2 * block)
        total = 0.0
        for h in range(heads):
            total = total + jnp.dot(att[h, rows, :], ow_ref[h], preferred_element_type=F32)
        part[0, t] = total[:block].astype(BF16)
        part[1, t] = total[block:].astype(BF16)
        return carry

    pair_copy = remote(part.at[1 - core], pair, pr_s, pr_r, {"tp": other})

    def add_pair(t, carry):
        chip_sum[t] = (part[core, t].astype(F32) + pair[t].astype(F32)).astype(BF16)
        return carry

    def line_copy(side, t, first):
        return remote(
            chip_sum.at[t] if first else line_out.at[side, t],
            landed.at[side, t],
            rs_s.at[side, t],
            rs_r.at[side, t],
            {"tp": (z + 1 - 2 * side) * 2 + core},
        )

    def stage_each(k, do):
        for side in range(2):
            at = k if side == 0 else chips - 1 - k
            targets = range(chips - 1, k, -1) if side == 0 else range(chips - 1 - k)

            @pl.when(z == at)
            def _(side=side, targets=targets):
                for t in targets:
                    do(side, t, k == 0)

    def stage_send(side, t, first):
        copy = line_copy(side, t, first)
        if not first:
            copy.wait_recv()
            line_out[side, t] = (
                chip_sum[t].astype(F32) + landed[side, t].astype(F32)
            ).astype(BF16)
        copy.start()

    def back_copy(c, s):
        return remote(
            back.at[c, pl.ds(s * cap, cap)],
            ret.at[c, pl.ds(s * cap, cap)],
            b_s.at[s],
            b_r.at[c],
            {"ep": lax.rem(me + ep - s, ep)},
        )

    def down_of(c):
        total = 0.0
        for src in range(chips):
            for i in range(subs):
                total = total + lax.dot_general(
                    hid[src, i, :half, :], w_dn[src, i, c], NT, preferred_element_type=F32
                )
        result = total.astype(BF16)
        ret[c, :cap, :] = result[:cap]
        back[c, cap:, :] = result[cap:]

    def combine(c):
        slots = pl.ds(cap, half - cap)
        remote(
            back.at[c, slots], ret.at[c, slots], b_s.at[0], b_r.at[c], {"tp": other}
        ).wait_recv()
        total = jnp.dot(take_ref[0], ret[c], preferred_element_type=F32)
        total = total + jnp.dot(take_ref[1], ret[c], preferred_element_type=F32)
        routed_ref[:, c * step : (c + 1) * step] = total.astype(BF16)

    def give_back(c):
        whole = w_dn.at[:, 0, c, :, pl.ds(unit, unit)] if subs == 1 else w_dn.at[:, 1, c]
        remote(whole, whole, sd_s.at[0], sd_r.at[c], {"tp": other}).wait_recv()
        down_of(c)
        for s in range(1, ep):
            back_copy(c, s).start()

    def own_hidden(first, last):
        lax.fori_loop(first, last, lambda src, carry: (hidden_of(src, 0, 2), carry)[1], 0)

    def guest_hidden(src):
        hidden_of(src, 2, 2)
        h_copy(src).start()

    def pass_rest(c, first=1):
        for k in range(first, chips):
            for near in (True, False):
                if k > 1 or near:
                    pass_dn(k, near, c)

    def start_mixed():
        lax.fori_loop(0, heads * tiles, finish, 0)
        own_ow.wait()
        lax.fori_loop(0, chips, project, 0)
        pair_copy.start()

    def chip_mixed():
        pair_copy.wait_recv()
        lax.fori_loop(0, chips, add_pair, 0)

    def attend_far():
        receive_far()
        for has, s in late_blocks:
            pl.when(has)(lambda s=s: attend(s))

    @pl.when(has_guest)
    def _():
        for copy in guest_copies():
            copy.wait_recv()
        dispatch(1)

    receive_near()
    send_far()
    for has, s in early_blocks:
        pl.when(has)(lambda s=s: attend(s))

    @pl.when(inner)
    def _():
        for j in range(PIECES):
            pass_gu(1, True, j)
        for j in range(PIECES - 1):
            pass_gu(1, False, j)
        for c in range(LATE, CHUNKS):
            pass_dn(1, True, c)
        ready_gu(z)
        ready_gu(z + inward)

    @pl.when(has_guest)
    def _():
        for s in range(1, ep):
            x_copy(1, s).wait_recv()
        guest_hidden(z)
        guest_hidden(z + inward)

    @pl.when(inner)
    def _():
        dispatch(0)
        pass_gu(1, False, PIECES - 1)
        ready_gu(z - inward)
        pl.when(has_guest)(lambda: guest_hidden(z - inward))
        for c in range(CHUNKS):
            if c == CHUNKS // 2:
                attend_far()
            if c < LATE:
                dn_copy(z, c, inward).start()
            pass_dn(1, False, c)
        for k in range(2, chips):
            for near in (True, False):
                for j in range(PIECES):
                    pass_gu(k, near, j)
                far = source(k, near)[0]

                @pl.when(on_line(far))
                def _(far=far):
                    ready_gu(far)
                    pl.when(has_guest)(lambda: guest_hidden(far))

        pass_rest(0)
        start_mixed()
        pass_rest(1)
        for s in range(1, ep):
            x_copy(0, s).wait_recv()
        own_hidden(0, chips // 2)
        pass_rest(2)
        own_hidden(chips // 2, chips)
        pass_rest(3)
        chip_mixed()
        for c in range(4):
            give_back(c)
        stage_each(1, stage_send)
        for c in range(4, CHUNKS):
            pass_rest(c, 1 if c < LATE else 2)
            give_back(c)

    @pl.when(is_end)
    def _():
        attend_far()
        start_mixed()
        chip_mixed()
        stage_each(0, stage_send)
        pass_rest(0)
        for src in range(chips):
            h_copy(src).wait_recv()
        give_back(0)
        for c in range(1, CHUNKS):
            pass_rest(c)
            give_back(c)

    for c in range(CHUNKS):
        if c == CHUNKS // 2:
            for k in range(2, chips - 1):
                stage_each(k, stage_send)
        combine(c)

    mixed_ref[...] = chip_sum[z]
    for side in range(2):

        @pl.when((z > 0) if side == 0 else (z < chips - 1))
        def _(side=side):
            line_copy(side, z, False).wait_recv()
            mixed_ref[...] = (
                mixed_ref[...].astype(F32) + landed[side, z].astype(F32)
            ).astype(BF16)

    for sends, s in near_sends:
        pl.when(sends)(lambda s=s: kv_copy(s).wait_send())
    if square_plane:
        pl.when(me == 1)(lambda: kv_lent().wait_send())
    for sends, copy in far_sends:
        pl.when(sends)(lambda copy=copy: copy().wait_send())
    for s in range(1, ep):

        @pl.when(inner)
        def _(s=s):
            x_copy(0, s).wait_send()

        @pl.when(has_guest)
        def _(s=s):
            x_copy(1, s).wait_send()

    @pl.when(is_end)
    def _():
        for copy in guest_copies():
            copy.wait_send()

    @pl.when(has_guest)
    def _():
        for src in range(chips):
            h_copy(src).wait_send()

    for k in range(chips):
        for near in (True, False):
            src, way = source(k, near)

            @pl.when(on_line(src))
            def _(k=k, near=near, src=src, way=way):
                @pl.when(wants_gu(z + way) & (inner | (k == 0)))
                def _():
                    gu_sent(src, way)

                @pl.when(on_line(z + way))
                def _():
                    dn_sent(src, way)

                if k or near:

                    @pl.when(inner)
                    def _():
                        sg_sent(src)

                    sd_sent(src)

    pair_copy.wait_send()
    for k in range(chips - 1):
        stage_each(k, lambda side, t, first: line_copy(side, t, first).wait_send())
    for s in range(1, ep):
        slots = pl.ds(s * cap, cap)
        remote(
            back.at[:, slots], ret.at[:, slots], b_s.at[s], b_r.at[0], {"tp": other}
        ).wait_send()


def per_device(
    queries,
    keys,
    values,
    mixing,
    head_gain,
    out_weight,
    tokens_b,
    norm_gain,
    expert_ids,
    group_gate,
    expert_gate,
    gate_weight,
    up_weight,
    down_weight,
):
    ep = lax.axis_size("ep")
    tp = lax.axis_size("tp")
    chips = tp // 2
    length, heads, wide = queries.shape
    val = values.shape[2]
    local_rows, width = tokens_b.shape
    top_count = expert_ids.shape[1]
    unit = gate_weight.shape[2]
    assert gate_weight.shape[0] == 1 and wide == 2 * HEAD and chips >= 4 and ep <= RANKS
    capacity = 3 * local_rows * top_count // (2 * ep)
    cap = -(-capacity // 16) * 16
    step = width // CHUNKS

    gate, up = gate_weight[0], up_weight[0]
    subs = 1
    if unit % 128:
        gate = jnp.concatenate([gate, up], axis=1)
        subs = 2
    half = ep * cap
    block = length // tp
    vmem = pl.BlockSpec(memory_space=pltpu.VMEM)
    anywhere = pl.BlockSpec(memory_space=pl.ANY)
    dma = pltpu.SemaphoreType.DMA
    return pl.pallas_call(
        functools.partial(kernel, ep, tp),
        out_shape=(
            pltpu.VMEM((block, width), BF16),
            pltpu.VMEM((local_rows, width), BF16),
        ),
        in_specs=[pl.BlockSpec(memory_space=pltpu.SMEM)] + [vmem] * 5 + [anywhere] * 8,
        out_specs=(vmem, vmem),
        scratch_shapes=[
            pltpu.VMEM((length, heads, wide), BF16),
            pltpu.VMEM((length, heads, wide), BF16),
            pltpu.VMEM((length, heads, val), BF16),
            pltpu.VMEM((heads, val, width), BF16),
            pltpu.VMEM((local_rows, width), BF16),
            pltpu.VMEM((heads, length, wide), BF16),
            pltpu.VMEM((ep, heads, length, wide + val), BF16),
            pltpu.VMEM((chips, width, 4 * unit), BF16),
            pltpu.VMEM((chips, subs, CHUNKS, step, 2 * unit // subs), BF16),
            pltpu.VMEM((2 * half, width), BF16),
            pltpu.VMEM((2, ep - 1, cap, width), BF16),
            pltpu.VMEM((2, local_rows, width), BF16),
            pltpu.VMEM((2, RANKS, local_rows), F32),
            pltpu.VMEM((chips, subs, 2 * half, 2 * unit // subs), BF16),
            pltpu.VMEM((CHUNKS, half, step), BF16),
            pltpu.VMEM((CHUNKS, half, step), BF16),
            pltpu.VMEM((2, heads, length, 1), F32),
            pltpu.VMEM((2, heads, length, 1), F32),
            pltpu.VMEM((2, heads, length, val), F32),
            pltpu.VMEM((heads, length, val), BF16),
            pltpu.VMEM((2, chips, block, width), BF16),
            pltpu.VMEM((chips, block, width), BF16),
            pltpu.VMEM((chips, block, width), BF16),
            pltpu.VMEM((2, chips, block, width), BF16),
            pltpu.VMEM((2, chips, block, width), BF16),
            pltpu.VMEM((2, local_rows, half), BF16),
            dma((8,)),
            dma((ep + 1,)),
            dma((ep + 1,)),
            dma((2,)),
            dma((2,)),
            dma((2, ep)),
            dma((2, ep)),
            dma((2, chips)),
            dma((chips, PIECES)),
            dma((chips,)),
            dma((chips, PIECES)),
            dma((2, chips)),
            dma((chips, CHUNKS)),
            dma((chips,)),
            dma((CHUNKS,)),
            dma((chips,)),
            dma((chips,)),
            dma,
            dma,
            dma((2, chips)),
            dma((2, chips)),
            dma((ep,)),
            dma((CHUNKS,)),
        ],
        compiler_params=pltpu.CompilerParams(
            collective_id=0, has_side_effects=True, vmem_limit_bytes=62 * 1024 * 1024
        ),
    )(
        mixing,
        head_gain[None],
        norm_gain[None],
        expert_ids.T,
        group_gate[None],
        expert_gate.T,
        queries,
        keys,
        values,
        out_weight,
        tokens_b,
        gate,
        up,
        down_weight[0].reshape(CHUNKS, step, unit),
    )


def solution(mesh):
    placed = (
        P("ep", "tp", None),
        P("ep", "tp", None),
        P("ep", "tp", None),
        P("tp"),
        P(),
        P("tp", None, None),
        P(("ep", "tp"), None),
        P(),
        P(("ep", "tp"), None),
        P(("ep", "tp")),
        P(("ep", "tp"), None),
        P("ep", None, "tp"),
        P("ep", None, "tp"),
        P("ep", None, "tp"),
    )
    return jax.shard_map(
        per_device,
        mesh=mesh,
        in_specs=placed,
        out_specs=(P(("ep", "tp"), None), P(("ep", "tp"), None)),
        check_vma=False,
    )
```

```python
import functools
import math

import jax
import jax.numpy as jnp
from jax import lax
from jax.experimental import pallas as pl
from jax.experimental.pallas import tpu as pltpu
from jax.sharding import PartitionSpec as P

HEAD = 64
CHUNKS = 8
LATE = 6
PIECES = 2
RANKS = 16
F32 = jnp.float32
BF16 = jnp.bfloat16
MESH = pl.DeviceIdType.MESH
NT = (((1,), (1,)), ((), ()))
TN = (((0,), (0,)), ((), ()))


def kernel(
    ep,
    tp,
    mix_ref,
    gain_ref,
    norm_ref,
    ids_ref,
    group_ref,
    gates_ref,
    q_in,
    k_in,
    v_in,
    ow_in,
    tok_in,
    gate_ref,
    up_ref,
    dn_ref,
    mixed_ref,
    routed_ref,
    q_raw,
    k_raw,
    v_raw,
    ow_ref,
    tok_ref,
    q_ref,
    kv_all,
    w_gu,
    w_dn,
    rows_x,
    out_ref,
    nrm,
    rank_ref,
    hid,
    back,
    ret,
    top_ref,
    sum_ref,
    val_ref,
    att,
    part,
    pair,
    chip_sum,
    landed,
    line_out,
    take_ref,
    local_sem,
    kv_s,
    kv_r,
    t_s,
    t_r,
    x_s,
    x_r,
    gu_s,
    gu_r,
    sg_s,
    sg_r,
    dn_s,
    dn_r,
    sd_s,
    sd_r,
    h_s,
    h_r,
    pr_s,
    pr_r,
    rs_s,
    rs_r,
    b_s,
    b_r,
):
    chips = tp // 2
    me = lax.axis_index("ep")
    mine = lax.axis_index("tp")
    z = mine // 2
    core = mine % 2
    other = z * 2 + 1 - core
    inward = 1 - 2 * (z // (chips // 2))
    heads, length, wide = q_ref.shape
    val = val_ref.shape[3]
    local_rows, width = tok_ref.shape
    half = rows_x.shape[0] // 2
    cap = half // ep
    step = w_dn.shape[3]
    lanes = w_gu.shape[2] // 2
    unit = lanes // 2
    subs = w_dn.shape[1]
    deep = width // PIECES
    joined = gate_ref.shape[1] != unit
    inner = (z >= 1) & (z <= chips - 2)
    is_end = (z == 0) | (z == chips - 1)
    has_guest = (z == 1) | (z == chips - 2)

    def remote(src, dst, send, recv, target):
        return pltpu.make_async_remote_copy(
            src_ref=src,
            dst_ref=dst,
            send_sem=send,
            recv_sem=recv,
            device_id=target,
            device_id_type=MESH,
        )

    if joined:
        own_gu = [pltpu.make_async_copy(gate_ref, w_gu.at[z, :, pl.ds(0, lanes)], local_sem.at[0])]
    else:
        own_gu = [
            pltpu.make_async_copy(gate_ref, w_gu.at[z, :, pl.ds(0, unit)], local_sem.at[0]),
            pltpu.make_async_copy(up_ref, w_gu.at[z, :, pl.ds(unit, unit)], local_sem.at[1]),
        ]
    if subs == 1:
        own_dn = pltpu.make_async_copy(dn_ref, w_dn.at[z, 0, :, :, pl.ds(0, unit)], local_sem.at[2])
    else:
        own_dn = pltpu.make_async_copy(dn_ref, w_dn.at[z, 0], local_sem.at[2])
    own_kv = [
        pltpu.make_async_copy(k_in, k_raw, local_sem.at[3]),
        pltpu.make_async_copy(v_in, v_raw, local_sem.at[4]),
        pltpu.make_async_copy(q_in, q_raw, local_sem.at[5]),
    ]
    own_tok = pltpu.make_async_copy(tok_in, tok_ref, local_sem.at[6])
    own_ow = pltpu.make_async_copy(ow_in, ow_ref, local_sem.at[7])

    barrier = pltpu.get_barrier_semaphore()
    for s in range(1, ep):
        pl.semaphore_signal(
            barrier, inc=1, device_id={"ep": (me + s) % ep}, device_id_type=MESH
        )
    pl.semaphore_signal(barrier, inc=1, device_id={"tp": other}, device_id_type=MESH)
    for way in (-1, 1):

        @pl.when((z + way >= 0) & (z + way <= chips - 1))
        def _(way=way):
            pl.semaphore_signal(
                barrier,
                inc=1,
                device_id={"tp": (z + way) * 2 + core},
                device_id_type=MESH,
            )

    for copy in [own_tok] + own_gu + own_kv + [own_dn, own_ow]:
        copy.start()
    on_sides = (z + chips - 1) // chips + (2 * chips - 2 - z) // chips
    pl.semaphore_wait(barrier, ep + on_sides)

    def on_line(at):
        return (at >= 0) & (at <= chips - 1)

    def wants_gu(at):
        return (at >= 1) & (at <= chips - 2)

    def gu_part(src, j):
        return w_gu.at[src, pl.ds(j * deep, deep), pl.ds(0, lanes)]

    def gu_copy(src, j, way):
        return remote(
            gu_part(src, j),
            gu_part(src, j),
            gu_s.at[(1 - way) // 2, src],
            gu_r.at[src, j],
            {"tp": (z + way) * 2 + core},
        )

    def sg_copy(src, j):
        return remote(
            gu_part(src, j),
            w_gu.at[src, pl.ds(j * deep, deep), pl.ds(lanes, lanes)],
            sg_s.at[src],
            sg_r.at[src, j],
            {"tp": other},
        )

    def dn_part(src, c, which):
        if subs == 1:
            return w_dn.at[src, 0, c, :, pl.ds(which * unit, unit)]
        return w_dn.at[src, which, c]

    def dn_copy(src, c, way):
        return remote(
            dn_part(src, c, 0),
            dn_part(src, c, 0),
            dn_s.at[(1 - way) // 2, src],
            dn_r.at[src, c],
            {"tp": (z + way) * 2 + core},
        )

    def sd_copy(src, c):
        return remote(
            dn_part(src, c, 0), dn_part(src, c, 1), sd_s.at[src], sd_r.at[c], {"tp": other}
        )

    def gu_sent(src, way):
        whole = w_gu.at[src, :, pl.ds(0, lanes)]
        sem = gu_s.at[(1 - way) // 2, src]
        remote(whole, whole, sem, gu_r.at[src, 0], {"tp": other}).wait_send()

    def sg_sent(src):
        whole = w_gu.at[src, :, pl.ds(0, lanes)]
        remote(whole, whole, sg_s.at[src], sg_r.at[src, 0], {"tp": other}).wait_send()

    def dn_whole(src):
        if subs == 1:
            return w_dn.at[src, 0, :, :, pl.ds(0, unit)]
        return w_dn.at[src, 0]

    def dn_sent(src, way):
        whole, sem = dn_whole(src), dn_s.at[(1 - way) // 2, src]
        remote(whole, whole, sem, dn_r.at[src, 0], {"tp": other}).wait_send()

    def sd_sent(src):
        whole = dn_whole(src)
        remote(whole, whole, sd_s.at[src], sd_r.at[0], {"tp": other}).wait_send()

    def start_own():
        for copy in own_gu:
            copy.wait()
        for way in (inward, -inward):

            @pl.when(wants_gu(z + way))
            def _(way=way):
                for j in range(PIECES):
                    gu_copy(z, j, way).start()

        @pl.when(inner)
        def _():
            for j in range(PIECES):
                sg_copy(z, j).start()

        own_dn.wait()

        @pl.when(is_end)
        def _():
            for c in range(CHUNKS):
                dn_copy(z, c, inward).start()

        @pl.when(inner)
        def _():
            for c in range(CHUNKS):
                dn_copy(z, c, -inward).start()
            for c in range(LATE, CHUNKS):
                dn_copy(z, c, inward).start()

        for c in range(CHUNKS):
            sd_copy(z, c).start()

    def source(k, near):
        return (z + k * inward, -inward) if near else (z - k * inward, inward)

    def pass_gu(k, near, j):
        src, way = source(k, near)

        @pl.when(inner & on_line(src))
        def _():
            gu_copy(src, j, way).wait_recv()
            pl.when(wants_gu(z + way))(lambda: gu_copy(src, j, way).start())
            sg_copy(src, j).start()

    def ready_gu(src):
        for j in range(PIECES):
            sg_copy(src, j).wait_recv()

    def pass_dn(k, near, c):
        src, way = source(k, near)

        @pl.when(on_line(src))
        def _():
            dn_copy(src, c, way).wait_recv()
            pl.when(on_line(z + way))(lambda: dn_copy(src, c, way).start())
            sd_copy(src, c).start()

    square_plane = ep == 4
    mid_rows = length // 2

    def kv_move(src, dst, sem, target):
        return remote(src, dst, kv_s.at[sem], kv_r.at[sem], {"ep": target})

    def kv_copy(s):
        return kv_move(kv_all.at[0], kv_all.at[s], s, lax.rem(me + s, ep))

    def kv_half(s, i):
        rows = pl.ds(i * mid_rows, mid_rows)
        return kv_move(kv_all.at[s, :, rows], kv_all.at[3, :, rows], 3 + i, 3)

    def kv_corner(s, i):
        rows = pl.ds(i * mid_rows, mid_rows)
        return kv_move(kv_all.at[s, :, rows], kv_all.at[1, :, rows], 3 + i, 2)

    def kv_lent():
        rows = pl.ds(mid_rows, mid_rows)
        return kv_move(kv_all.at[0, :, rows], kv_all.at[1, :, rows], 1, 0)

    if square_plane:
        near_sends = [((me == 0) | (me == 2), 1), (me <= 1, 2)]
        far_sends = [
            (me == 1, lambda: kv_half(1, 0)),
            (me == 2, lambda: kv_half(2, 1)),
            (me == 3, lambda: kv_corner(2, 0)),
            (me == 0, lambda: kv_corner(1, 1)),
        ]
        early_blocks = [((me == 1) | (me == 3), 1), (me >= 2, 2)]
        late_blocks = [(me >= 2, jnp.where(me == 2, 1, 3))]
    else:
        near_sends = [(me + s < ep, s) for s in range(1, ep - 1)]
        far_sends = [(me + ep - 1 < ep, lambda: kv_copy(ep - 1))]
        early_blocks = [(me >= s, s) for s in range(1, ep - 1)]
        late_blocks = [(me >= ep - 1, ep - 1)]

    def send_near():
        for sends, s in near_sends:
            pl.when(sends)(lambda s=s: kv_copy(s).start())
        if square_plane:
            pl.when(me == 1)(lambda: kv_lent().start())

    def receive_near():
        for has, s in early_blocks:
            pl.when(has)(lambda s=s: kv_copy(s).wait_recv())
        if square_plane:
            pl.when(me == 0)(lambda: kv_lent().wait_recv())

    def send_far():
        for sends, copy in far_sends:
            pl.when(sends)(lambda copy=copy: copy().start())

    def receive_far():
        if square_plane:

            @pl.when(me == 2)
            def _():
                kv_corner(2, 0).wait_recv()
                kv_corner(1, 1).wait_recv()

            @pl.when(me == 3)
            def _():
                kv_half(1, 0).wait_recv()
                kv_half(2, 1).wait_recv()

        else:
            pl.when(me >= ep - 1)(lambda: kv_copy(ep - 1).wait_recv())

    pl.when(inner)(start_own)
    own_tok.wait()

    relative = ids_ref[...] - me
    relative = jnp.where(relative < 0, relative + ep, relative)
    table = (RANKS, local_rows)
    expert_row = lax.broadcasted_iota(jnp.int32, table, 0)
    named = jnp.zeros(table, F32)
    route = jnp.zeros(table, F32)
    for k in range(ids_ref.shape[0]):
        hit = expert_row == relative[k : k + 1, :]
        named = jnp.where(hit, 1.0, named)
        route = route + jnp.where(hit, group_ref[...] * gates_ref[k : k + 1, :], 0.0)
    square = (local_rows, local_rows)
    row_at = lax.broadcasted_iota(jnp.int32, square, 0)
    col_at = lax.broadcasted_iota(jnp.int32, square, 1)
    before = jnp.where(row_at < col_at, 1.0, 0.0).astype(BF16)
    rank = jnp.dot(named.astype(BF16), before, preferred_element_type=F32)
    rank_ref[0] = jnp.where(named > 0.5, rank, -1.0)
    tokens = tok_ref[...].astype(F32)
    nrm[0] = (
        tokens
        * lax.rsqrt(jnp.mean(tokens * tokens, axis=1, keepdims=True) + 1e-06)
        * norm_ref[...]
    ).astype(BF16)

    def guest_copies():
        target = {"tp": (z + inward) * 2 + core}
        return (
            remote(nrm.at[0], nrm.at[1], t_s.at[0], t_r.at[0], target),
            remote(rank_ref.at[0], rank_ref.at[1], t_s.at[1], t_r.at[1], target),
        )

    @pl.when(is_end)
    def _():
        for copy in guest_copies():
            copy.start()
        start_own()

    for copy in own_kv:
        copy.wait()
    part_rows = min(128, length)

    def lay_kv(t, carry):
        rows = pl.ds(pl.multiple_of(t * part_rows, part_rows), part_rows)
        k_flat = k_raw[rows].reshape(part_rows, heads * wide)
        v_flat = v_raw[rows].reshape(part_rows, heads * val)
        for h in range(heads):
            kv_all[0, h, rows, :wide] = k_flat[:, h * wide : (h + 1) * wide]
            kv_all[0, h, rows, wide:] = v_flat[:, h * val : (h + 1) * val]
        return carry

    def lay_q(t, carry):
        rows = pl.ds(pl.multiple_of(t * part_rows, part_rows), part_rows)
        q_flat = q_raw[rows].reshape(part_rows, heads * wide)
        for h in range(heads):
            q = q_flat[:, h * wide : (h + 1) * wide].astype(F32) * (1.0 / math.sqrt(HEAD))
            q_ref[h, rows, :] = q.astype(BF16)
        return carry

    lax.fori_loop(0, length // part_rows, lay_kv, 0)
    send_near()
    lax.fori_loop(0, length // part_rows, lay_q, 0)

    def x_copy(g, s):
        return remote(
            out_ref.at[g, s - 1],
            rows_x.at[pl.ds(g * half + s * cap, cap)],
            x_s.at[g],
            x_r.at[g],
            {"ep": lax.rem(me + s, ep)},
        )

    def x_whole(g):
        whole = rows_x.at[pl.ds(g * half + cap, half - cap)]
        return remote(whole, whole, x_s.at[g], x_r.at[g], {"tp": other})

    slot_row = lax.broadcasted_iota(jnp.int32, (cap, local_rows), 0).astype(F32)

    def place_of(g, s):
        return jnp.where(rank_ref[g, s : s + 1, :] == slot_row, 1.0, 0.0).astype(BF16)

    def dispatch(g):
        for s in list(range(1, ep)) + [0]:
            place = place_of(g, s)
            for n in range(CHUNKS):
                cols = slice(n * step, (n + 1) * step)
                picked = jnp.dot(place, nrm[g, :, cols], preferred_element_type=F32).astype(BF16)
                if s:
                    out_ref[g, s - 1, :, cols] = picked
                else:
                    rows_x[g * half : g * half + cap, cols] = picked
            if s:
                x_copy(g, s).start()

    tile = min(256, length)
    tiles = length // tile

    def attend(s, first=False):
        block = kv_all.at[s]

        def one(index, carry):
            h = index // tiles
            start = pl.multiple_of((index % tiles) * tile, tile)
            rows = pl.ds(start, tile)
            q = q_ref[h, rows, :]
            lane = lax.broadcasted_iota(jnp.int32, (tile, wide), 1)
            for m in range(2):
                pick = (lane < HEAD) if m == 0 else (lane >= HEAD)
                q_map = jnp.where(pick, q, jnp.zeros_like(q))
                scores = lax.dot_general(q_map, block[h, :, :wide], NT, preferred_element_type=F32)
                if first:
                    row = start + lax.broadcasted_iota(jnp.int32, scores.shape, 0)
                    col = lax.broadcasted_iota(jnp.int32, scores.shape, 1)
                    scores = jnp.where(col <= row, scores, -1e30)
                    fresh = jnp.max(scores, axis=1, keepdims=True)
                else:
                    top = top_ref[m, h, rows, :]
                    fresh = jnp.maximum(top, jnp.max(scores, axis=1, keepdims=True))
                expo = jnp.exp(scores - fresh)
                total = jnp.sum(expo, axis=1, keepdims=True)
                value = jnp.dot(
                    expo.astype(BF16), block[h, :, wide:], preferred_element_type=F32
                )
                if not first:
                    shrink = jnp.exp(top - fresh)
                    total = total + sum_ref[m, h, rows, :] * shrink
                    value = value + val_ref[m, h, rows, :] * shrink
                top_ref[m, h, rows, :] = fresh
                sum_ref[m, h, rows, :] = total
                val_ref[m, h, rows, :] = value
            return carry

        lax.fori_loop(0, heads * tiles, one, 0)

    attend(0, True)

    slot_at = lax.broadcasted_iota(jnp.int32, (local_rows, half), 1).astype(F32)
    weight = jnp.zeros((local_rows, half), F32)
    diagonal = row_at == col_at
    for s in range(ep):
        rank_col = jnp.sum(jnp.where(diagonal, rank_ref[0, s : s + 1, :], 0.0), axis=1, keepdims=True)
        route_col = jnp.sum(jnp.where(diagonal, route[s : s + 1, :], 0.0), axis=1, keepdims=True)
        lane_of = jnp.where(rank_col >= 0.0, rank_col + float(s * cap), -1.0)
        weight = jnp.where(slot_at == lane_of, route_col, weight)
    upper = weight.astype(BF16)
    take_ref[0] = upper
    take_ref[1] = (weight - upper.astype(F32)).astype(BF16)

    m_tile = half // 2

    def hidden_of(src, first, count):
        def one(t, carry):
            rows = pl.ds(pl.multiple_of(t * m_tile, m_tile), m_tile)
            product = jnp.dot(rows_x[rows, :], w_gu[src], preferred_element_type=F32)
            for i in range(2):
                gate = product[:, i * lanes : i * lanes + unit]
                value = gate / (1.0 + jnp.exp(-gate)) * product[:, i * lanes + unit : (i + 1) * lanes]
                if subs == 1:
                    hid[src, 0, rows, i * unit : (i + 1) * unit] = value.astype(BF16)
                else:
                    hid[src, i, rows, :] = value.astype(BF16)
            return carry

        lax.fori_loop(first, first + count, one, 0)

    def h_copy(src):
        return remote(
            hid.at[src, :, pl.ds(half, half)],
            hid.at[src, :, pl.ds(0, half)],
            h_s,
            h_r,
            {"tp": (z - inward) * 2 + core},
        )

    def finish(index, carry):
        h = index // tiles
        rows = pl.ds(pl.multiple_of((index % tiles) * tile, tile), tile)
        diff = val_ref[0, h, rows, :] / sum_ref[0, h, rows, :] - mix_ref[h] * (
            val_ref[1, h, rows, :] / sum_ref[1, h, rows, :]
        )
        scaled = diff * lax.rsqrt(jnp.mean(diff * diff, axis=1, keepdims=True) + 1e-05)
        att[h, rows, :] = (scaled * gain_ref[...]).astype(BF16)
        return carry

    block = length // tp

    def project(t, carry):
        rows = pl.ds(pl.multiple_of(t * 2 * block, 2 * block), 2 * block)
        total = 0.0
        for h in range(heads):
            total = total + jnp.dot(att[h, rows, :], ow_ref[h], preferred_element_type=F32)
        part[0, t] = total[:block].astype(BF16)
        part[1, t] = total[block:].astype(BF16)
        return carry

    pair_copy = remote(part.at[1 - core], pair, pr_s, pr_r, {"tp": other})

    def add_pair(t, carry):
        chip_sum[t] = (part[core, t].astype(F32) + pair[t].astype(F32)).astype(BF16)
        return carry

    def line_copy(side, t, first):
        return remote(
            chip_sum.at[t] if first else line_out.at[side, t],
            landed.at[side, t],
            rs_s.at[side, t],
            rs_r.at[side, t],
            {"tp": (z + 1 - 2 * side) * 2 + core},
        )

    def stage_each(k, do):
        for side in range(2):
            at = k if side == 0 else chips - 1 - k
            targets = range(chips - 1, k, -1) if side == 0 else range(chips - 1 - k)

            @pl.when(z == at)
            def _(side=side, targets=targets):
                for t in targets:
                    do(side, t, k == 0)

    def stage_send(side, t, first):
        copy = line_copy(side, t, first)
        if not first:
            copy.wait_recv()
            line_out[side, t] = (
                chip_sum[t].astype(F32) + landed[side, t].astype(F32)
            ).astype(BF16)
        copy.start()

    def back_copy(c, s):
        return remote(
            back.at[c, pl.ds(s * cap, cap)],
            ret.at[c, pl.ds(s * cap, cap)],
            b_s.at[s],
            b_r.at[c],
            {"ep": lax.rem(me + ep - s, ep)},
        )

    def down_of(c):
        total = 0.0
        for src in range(chips):
            for i in range(subs):
                total = total + lax.dot_general(
                    hid[src, i, :half, :], w_dn[src, i, c], NT, preferred_element_type=F32
                )
        result = total.astype(BF16)
        ret[c, :cap, :] = result[:cap]
        back[c, cap:, :] = result[cap:]

    def combine(c):
        slots = pl.ds(cap, half - cap)
        remote(
            back.at[c, slots], ret.at[c, slots], b_s.at[0], b_r.at[c], {"tp": other}
        ).wait_recv()
        total = jnp.dot(take_ref[0], ret[c], preferred_element_type=F32)
        total = total + jnp.dot(take_ref[1], ret[c], preferred_element_type=F32)
        routed_ref[:, c * step : (c + 1) * step] = total.astype(BF16)

    def give_back(c):
        whole = w_dn.at[:, 0, c, :, pl.ds(unit, unit)] if subs == 1 else w_dn.at[:, 1, c]
        remote(whole, whole, sd_s.at[0], sd_r.at[c], {"tp": other}).wait_recv()
        down_of(c)
        for s in range(1, ep):
            back_copy(c, s).start()

    def own_hidden(first, last):
        lax.fori_loop(first, last, lambda src, carry: (hidden_of(src, 0, 2), carry)[1], 0)

    def guest_hidden(src):
        hidden_of(src, 2, 2)
        h_copy(src).start()

    def pass_rest(c, first=1):
        for k in range(first, chips):
            for near in (True, False):
                if k > 1 or near:
                    pass_dn(k, near, c)

    def start_mixed():
        lax.fori_loop(0, heads * tiles, finish, 0)
        own_ow.wait()
        lax.fori_loop(0, chips, project, 0)
        pair_copy.start()

    def chip_mixed():
        pair_copy.wait_recv()
        lax.fori_loop(0, chips, add_pair, 0)

    def attend_far():
        receive_far()
        for has, s in late_blocks:
            pl.when(has)(lambda s=s: attend(s))

    @pl.when(has_guest)
    def _():
        for copy in guest_copies():
            copy.wait_recv()
        dispatch(1)

    def h_whole():
        whole = hid.at[:, :, pl.ds(0, half)]
        return remote(whole, whole, h_s, h_r, {"tp": other})

    receive_near()
    send_far()
    for has, s in early_blocks:
        pl.when(has)(lambda s=s: attend(s))

    @pl.when(inner)
    def _():
        for j in range(PIECES):
            pass_gu(1, True, j)
        for j in range(PIECES - 1):
            pass_gu(1, False, j)
        for c in range(LATE, CHUNKS):
            pass_dn(1, True, c)
        ready_gu(z)
        ready_gu(z + inward)

    @pl.when(has_guest)
    def _():
        x_whole(1).wait_recv()
        guest_hidden(z)
        guest_hidden(z + inward)

    @pl.when(inner)
    def _():
        dispatch(0)
        pass_gu(1, False, PIECES - 1)
        ready_gu(z - inward)
        pl.when(has_guest)(lambda: guest_hidden(z - inward))
        for c in range(CHUNKS):
            if c == CHUNKS // 2:
                attend_far()
            if c < LATE:
                dn_copy(z, c, inward).start()
            pass_dn(1, False, c)
        for k in range(2, chips):
            for near in (True, False):
                for j in range(PIECES):
                    pass_gu(k, near, j)
                far = source(k, near)[0]

                @pl.when(on_line(far))
                def _(far=far):
                    ready_gu(far)
                    pl.when(has_guest)(lambda: guest_hidden(far))

        pass_rest(0)
        start_mixed()
        pass_rest(1)
        x_whole(0).wait_recv()
        own_hidden(0, chips // 2)
        pass_rest(2)
        own_hidden(chips // 2, chips)
        pass_rest(3)
        chip_mixed()
        for c in range(4):
            give_back(c)
        stage_each(1, stage_send)
        for c in range(4, CHUNKS):
            pass_rest(c, 1 if c < LATE else 2)
            give_back(c)

    @pl.when(is_end)
    def _():
        attend_far()
        start_mixed()
        chip_mixed()
        stage_each(0, stage_send)
        pass_rest(0)
        h_whole().wait_recv()
        give_back(0)
        for c in range(1, CHUNKS):
            pass_rest(c)
            give_back(c)

    for c in range(CHUNKS):
        if c == CHUNKS // 2:
            for k in range(2, chips - 1):
                stage_each(k, stage_send)
        combine(c)

    mixed_ref[...] = chip_sum[z]
    for side in range(2):

        @pl.when((z > 0) if side == 0 else (z < chips - 1))
        def _(side=side):
            line_copy(side, z, False).wait_recv()
            mixed_ref[...] = (
                mixed_ref[...].astype(F32) + landed[side, z].astype(F32)
            ).astype(BF16)

    for sends, s in near_sends:
        pl.when(sends)(lambda s=s: kv_copy(s).wait_send())
    if square_plane:
        pl.when(me == 1)(lambda: kv_lent().wait_send())
    for sends, copy in far_sends:
        pl.when(sends)(lambda copy=copy: copy().wait_send())
    pl.when(inner)(lambda: x_whole(0).wait_send())
    pl.when(has_guest)(lambda: x_whole(1).wait_send())

    @pl.when(is_end)
    def _():
        for copy in guest_copies():
            copy.wait_send()

    @pl.when(has_guest)
    def _():
        h_whole().wait_send()

    for k in range(chips):
        for near in (True, False):
            src, way = source(k, near)

            @pl.when(on_line(src))
            def _(k=k, near=near, src=src, way=way):
                @pl.when(wants_gu(z + way) & (inner | (k == 0)))
                def _():
                    gu_sent(src, way)

                @pl.when(on_line(z + way))
                def _():
                    dn_sent(src, way)

                if k or near:

                    @pl.when(inner)
                    def _():
                        sg_sent(src)

                    sd_sent(src)

    pair_copy.wait_send()
    for k in range(chips - 1):
        stage_each(k, lambda side, t, first: line_copy(side, t, first).wait_send())
    for s in range(1, ep):
        slots = pl.ds(s * cap, cap)
        remote(
            back.at[:, slots], ret.at[:, slots], b_s.at[s], b_r.at[0], {"tp": other}
        ).wait_send()


def per_device(
    queries,
    keys,
    values,
    mixing,
    head_gain,
    out_weight,
    tokens_b,
    norm_gain,
    expert_ids,
    group_gate,
    expert_gate,
    gate_weight,
    up_weight,
    down_weight,
):
    ep = lax.axis_size("ep")
    tp = lax.axis_size("tp")
    chips = tp // 2
    length, heads, wide = queries.shape
    val = values.shape[2]
    local_rows, width = tokens_b.shape
    top_count = expert_ids.shape[1]
    unit = gate_weight.shape[2]
    assert gate_weight.shape[0] == 1 and wide == 2 * HEAD and chips >= 4 and ep <= RANKS
    capacity = 3 * local_rows * top_count // (2 * ep)
    cap = -(-capacity // 16) * 16
    step = width // CHUNKS

    gate, up = gate_weight[0], up_weight[0]
    subs = 1
    if unit % 128:
        gate = jnp.concatenate([gate, up], axis=1)
        subs = 2
    half = ep * cap
    block = length // tp
    vmem = pl.BlockSpec(memory_space=pltpu.VMEM)
    anywhere = pl.BlockSpec(memory_space=pl.ANY)
    dma = pltpu.SemaphoreType.DMA
    return pl.pallas_call(
        functools.partial(kernel, ep, tp),
        out_shape=(
            pltpu.VMEM((block, width), BF16),
            pltpu.VMEM((local_rows, width), BF16),
        ),
        in_specs=[pl.BlockSpec(memory_space=pltpu.SMEM)] + [vmem] * 5 + [anywhere] * 8,
        out_specs=(vmem, vmem),
        scratch_shapes=[
            pltpu.VMEM((length, heads, wide), BF16),
            pltpu.VMEM((length, heads, wide), BF16),
            pltpu.VMEM((length, heads, val), BF16),
            pltpu.VMEM((heads, val, width), BF16),
            pltpu.VMEM((local_rows, width), BF16),
            pltpu.VMEM((heads, length, wide), BF16),
            pltpu.VMEM((ep, heads, length, wide + val), BF16),
            pltpu.VMEM((chips, width, 4 * unit), BF16),
            pltpu.VMEM((chips, subs, CHUNKS, step, 2 * unit // subs), BF16),
            pltpu.VMEM((2 * half, width), BF16),
            pltpu.VMEM((2, ep - 1, cap, width), BF16),
            pltpu.VMEM((2, local_rows, width), BF16),
            pltpu.VMEM((2, RANKS, local_rows), F32),
            pltpu.VMEM((chips, subs, 2 * half, 2 * unit // subs), BF16),
            pltpu.VMEM((CHUNKS, half, step), BF16),
            pltpu.VMEM((CHUNKS, half, step), BF16),
            pltpu.VMEM((2, heads, length, 1), F32),
            pltpu.VMEM((2, heads, length, 1), F32),
            pltpu.VMEM((2, heads, length, val), F32),
            pltpu.VMEM((heads, length, val), BF16),
            pltpu.VMEM((2, chips, block, width), BF16),
            pltpu.VMEM((chips, block, width), BF16),
            pltpu.VMEM((chips, block, width), BF16),
            pltpu.VMEM((2, chips, block, width), BF16),
            pltpu.VMEM((2, chips, block, width), BF16),
            pltpu.VMEM((2, local_rows, half), BF16),
            dma((8,)),
            dma((ep + 1,)),
            dma((ep + 1,)),
            dma((2,)),
            dma((2,)),
            dma((2,)),
            dma((2,)),
            dma((2, chips)),
            dma((chips, PIECES)),
            dma((chips,)),
            dma((chips, PIECES)),
            dma((2, chips)),
            dma((chips, CHUNKS)),
            dma((chips,)),
            dma((CHUNKS,)),
            dma,
            dma,
            dma,
            dma,
            dma((2, chips)),
            dma((2, chips)),
            dma((ep,)),
            dma((CHUNKS,)),
        ],
        compiler_params=pltpu.CompilerParams(
            collective_id=0, has_side_effects=True, vmem_limit_bytes=62 * 1024 * 1024
        ),
    )(
        mixing,
        head_gain[None],
        norm_gain[None],
        expert_ids.T,
        group_gate[None],
        expert_gate.T,
        queries,
        keys,
        values,
        out_weight,
        tokens_b,
        gate,
        up,
        down_weight[0].reshape(CHUNKS, step, unit),
    )


def solution(mesh):
    placed = (
        P("ep", "tp", None),
        P("ep", "tp", None),
        P("ep", "tp", None),
        P("tp"),
        P(),
        P("tp", None, None),
        P(("ep", "tp"), None),
        P(),
        P(("ep", "tp"), None),
        P(("ep", "tp")),
        P(("ep", "tp"), None),
        P("ep", None, "tp"),
        P("ep", None, "tp"),
        P("ep", None, "tp"),
    )
    return jax.shard_map(
        per_device,
        mesh=mesh,
        in_specs=placed,
        out_specs=(P(("ep", "tp"), None), P(("ep", "tp"), None)),
        check_vma=False,
    )
```
